128 devices in a mesh: ep: 64 (over z, y, x), tp: 2 (over core).
Axes of the slice: x: 4, y: 4, z: 4, core: 2. Of those that a mesh axis runs over, the one named last changes fastest.
Arguments:
- tokens: bfloat16 [1024, 2048], P('ep'), may hold values from -6 to 6
- attn_gain: float32 [2048], replicated, may hold values from 0.1 to 1.9
- w_query1: bfloat16 [2048, 512], P(None, 'tp'), may hold values from -0.125 to 0.125
- w_query2: bfloat16 [2048, 512], P(None, 'tp'), may hold values from -0.125 to 0.125
- w_key1: bfloat16 [2048, 128], P(None, 'tp'), may hold values from -0.125 to 0.125
- w_key2: bfloat16 [2048, 128], P(None, 'tp'), may hold values from -0.125 to 0.125
- w_value: bfloat16 [2048, 256], P(None, 'tp'), may hold values from -0.125 to 0.125
- query_gain: float32 [64], replicated, may hold values from 1.1 to 1.6
- key_gain: float32 [64], replicated, may hold values from 1.1 to 1.6
- head_lambda: float32 [8], P('tp'), may hold values from 0.3 to 0.8
- sub_gain: float32 [128], replicated, may hold values from 0.1 to 1.9
- w_output: bfloat16 [1024, 2048], P('tp'), may hold values from -0.1875 to 0.1875
- cache_key: bfloat16 [1024, 2, 1024, 128], P('ep', 'tp'), may hold values from -300 to 300
- cache_value: bfloat16 [1024, 2, 1024, 128], P('ep', 'tp'), may hold values from -6 to 6
- lengths: int32 [1024], P('ep'), may hold values from 1 to 1024, 524288 in all
- mix_gain: float32 [2048], replicated, may hold values from 0.1 to 1.9
- expert_gate: bfloat16 [64, 2048, 1536], P('ep', None, 'tp'), may hold values from -0.375 to 0.375
- expert_up: bfloat16 [64, 2048, 1536], P('ep', None, 'tp'), may hold values from -0.375 to 0.375
- expert_down: bfloat16 [64, 1536, 2048], P('ep', 'tp'), may hold values from -0.0546875 to 0.0546875
- routes: int32 [1024, 4], P('ep'), may hold values from 0 to 63, all different within a row; in each aligned block of 16 rows (0 to 15, 16 to 31, ...) at most 2 rows name the same one
- route_weight: bfloat16 [1024, 4], P('ep'), may hold values from 0.049804688 to 0.59765625
- dense_mix: bfloat16 [2048], replicated, may hold values from -0.125 to 0.125
- dense_gate: bfloat16 [2048, 4096], P(None, ('ep', 'tp')), may hold values from -0.375 to 0.375
- dense_up: bfloat16 [2048, 4096], P(None, ('ep', 'tp')), may hold values from -0.375 to 0.375
- dense_down: bfloat16 [4096, 2048], P(('ep', 'tp')), may hold values from -0.03125 to 0.03125
Outputs:
- layer_out: bfloat16 [1024, 2048], P('ep', 'tp')
The draws below stay inside these ranges and needn't reach their ends.
Inputs may be any that keep to these rules, and one draw needn't show every extreme that they name: `lengths`: each sequence has at least one cached position in use; some sequence uses all 1024. `routes`: each row names 4 different experts; among the rows of one index of ep no expert is named by more than 2 rows, and in some such block one expert is named by exactly 2.
All inputs are finite; a program needn't handle non-finite values. No bound on the sum of `lengths` on one device may be relied on, other than what follows from the above.
Results may differ from the reference program's by a relative error of at most 0.018.
The reference program's roundings to bfloat16 on the way count: a program that leaves them out, or rounds other values in their place, can miss the bound.
Values may be sent and summed in bfloat16 or wider, within the bound.
No kernel may reach another device: no remote copies, remote signals or barrier semaphores. Data moves between devices by JAX's collectives and lax.ppermute only.
A program may use at most 128 MiB of HBM per device.

```python
import math
import jax
import jax.numpy as jnp
import numpy as np
from jax import lax

D = 2048
HEADS = 8
KV_HEADS = 2
HEAD = 64
VHEAD = 128
FF = 1536
DENSE_FF = 4096
TOP_K = 4
SEQS_DEV = 16
CACHE = 1024
EXPERTS = 64
CAP = 2
SEQS = 1024
N_EP = 64
N_TP = 2


def draw_cache_key(key, part):
    base = jax.random.normal(key, (SEQS, KV_HEADS, CACHE, 2 * HEAD), jnp.float32) * 1.35
    base = jnp.clip(base, -8.0, 8.0)
    return base.astype(jnp.bfloat16)


def level_of(key, extent, cuts, least, top_value):
    loudness, own = 1.0, jax.random.fold_in(key, 6)
    for position, blocks in cuts:
        steps = jnp.exp(jax.random.uniform(jax.random.fold_in(own, position), (blocks,), jnp.float32, least / len(cuts), top_value / len(cuts)))
        loudness = loudness * jnp.repeat(steps, extent[position] // blocks).reshape([-1 if axis == position else 1 for axis in range(len(extent))])
    return loudness


def split_up(count, total, most, slope):
    loads = [(1 << 20) // math.isqrt(rank ** slope) + 1 for rank in range(2, count + 1)]
    rest, holding = total - most - (count - 1), [1] * (count - 1)
    while rest > 0:
        movable = [i for i in range(count - 1) if holding[i] < most]
        mass, left = sum([loads[i] for i in movable]), rest
        for i in movable:
            addition = min(most - holding[i], max(1, left * loads[i] // mass), rest)
            holding[i] = holding[i] + addition
            rest = rest - addition
    return np.array([most] + holding)


def uneven_parts(key, count, total, bound, lean):
    if count == 2:
        one = jax.random.randint(key, (), max(1, total - bound), min(bound, total - 1) + 1)
        return jnp.stack([one, total - one])
    tallies = jnp.asarray(split_up(count, total, bound, lean), jnp.int32)
    twos = (count - 1) // 2
    source_of, sink = tallies[1:1 + 2 * twos:2], tallies[2:2 + 2 * twos:2]
    room = jnp.minimum(source_of - 1, bound - sink)
    shifted = jax.random.randint(jax.random.fold_in(key, 1), (twos,), 0, 1 << 20) % (room + 1)
    tallies = tallies.at[1:1 + 2 * twos:2].set(source_of - shifted).at[2:2 + 2 * twos:2].set(sink + shifted)
    return tallies[jax.random.permutation(jax.random.fold_in(key, 2), count)]


def shared_out(own_key, own, number, rows, number_of, top, most, skew):
    ranking = jax.random.permutation(own_key, number_of)
    crowded, usual = load_shares(number_of, rows * top, most, skew, True), load_shares(number_of, rows * top, most, skew, False)
    places = jnp.arange(number_of)

    def named(sizes, turn):
        used = int((sizes > 0).sum())
        fixed = max(1, used // 4)
        moved = fixed + (places - fixed + turn * (used - fixed)) % max(1, number_of - fixed)
        return jnp.zeros((number_of,), jnp.int32).at[ranking[jnp.where(places < fixed, places, moved)]].set(jnp.asarray(sizes, jnp.int32))

    sizes = jnp.where(number % 4 == 0, named(crowded, number // 4), named(usual, number - number // 4 - 1))
    mixed = jax.random.permutation(jax.random.fold_in(own, 3), number_of)
    donor, sink = mixed[0:number_of // 2 * 2:2], mixed[1:number_of // 2 * 2:2]
    room = jnp.minimum(sizes[donor] - 1, most - sizes[sink]) // 2
    room = jnp.where((donor == ranking[0]) | (sink == ranking[0]) | (sizes[sink] == 0), 0, jnp.maximum(room, 0))
    moved = jax.random.randint(jax.random.fold_in(own, 4), (number_of // 2,), 0, 1 << 20) % (room + 1)
    sizes = sizes.at[donor].add(-moved).at[sink].add(moved)
    members = jnp.searchsorted(jnp.cumsum(sizes), jnp.arange(rows * top), side="right").astype(jnp.int32)
    grid = members.reshape(top, rows).T
    grid = grid[jax.random.permutation(jax.random.fold_in(own, 1), rows)]
    turn = jax.random.randint(jax.random.fold_in(own, 2), (rows, 1), 0, top)
    return jnp.take_along_axis(grid, (jnp.arange(top)[None, :] + turn) % top, axis=1)


def load_shares(number_of, total, reach, slope, full):
    weights = [(1 << 20) // math.isqrt(grade ** slope) + 1 for grade in range(1, number_of + 1)]
    largest = reach if full else min(reach, max(-(-total // number_of), total * weights[0] // sum(weights)))
    least = 1 if total - largest >= number_of - 1 else 0
    holding, spare = [largest] + [least] * (number_of - 1), total - largest - least * (number_of - 1)
    while spare > 0:
        free = [i for i in range(1, number_of) if holding[i] < largest] or [i for i in range(1, number_of) if holding[i] < reach]
        mass, left = sum([weights[i] for i in free]), spare
        for i in free:
            addition = min(reach - holding[i], max(1, left * weights[i] // mass), spare)
            holding[i] = holding[i] + addition
            spare = spare - addition
    return np.array(holding)


def gaussian(key, shape, width, bound, split=(), kind=jnp.bfloat16):
    result = width * jax.random.normal(key, shape, jnp.float32)
    if split:
        result = result * level_of(key, shape, split, -0.22, 0.18)
    return jnp.clip(result, -bound, bound).astype(kind)


def setup_inputs(seed: int = 0) -> dict:
    splits = jax.random.split(jax.random.key(seed), 26)
    tokens = gaussian(splits[0], (SEQS, D), 1.0, 6.0, ((0, 64),))
    attn_gain = jnp.clip(1.0 + 0.18 * jax.random.normal(splits[1], (D,), jnp.float32), 0.1, 1.9)
    w_query1 = gaussian(splits[2], (D, HEADS * HEAD), D ** -0.5, 0.125, ((1, 2),))
    w_query2 = gaussian(splits[3], (D, HEADS * HEAD), D ** -0.5, 0.125, ((1, 2),))
    w_key1 = gaussian(splits[4], (D, KV_HEADS * HEAD), D ** -0.5, 0.125, ((1, 2),))
    w_key2 = gaussian(splits[5], (D, KV_HEADS * HEAD), D ** -0.5, 0.125, ((1, 2),))
    w_value = gaussian(splits[6], (D, KV_HEADS * VHEAD), D ** -0.5, 0.125, ((1, 2),))
    query_gain = jnp.clip(jax.random.uniform(splits[7], (HEAD,), jnp.float32, 1.1, 1.6), 1.1, 1.6)
    key_gain = jnp.clip(jax.random.uniform(splits[8], (HEAD,), jnp.float32, 1.1, 1.6), 1.1, 1.6)
    head_lambda = jnp.clip(0.3 + 0.5 * jax.random.uniform(splits[9], (HEADS,), jnp.float32) ** level_of(splits[9], (HEADS,), ((0, 2),), -0.2, 0.2), 0.3, 0.8)
    sub_gain = jnp.clip(1.0 + 0.18 * jax.random.normal(splits[10], (VHEAD,), jnp.float32), 0.1, 1.9)
    w_output = gaussian(splits[11], (HEADS * VHEAD, D), (HEADS * VHEAD) ** -0.5, 0.1875, ((0, 2),))
    cache_key = draw_cache_key(jax.random.fold_in(splits[25], 71), 0)
    cache_value = gaussian(splits[13], (SEQS, KV_HEADS, CACHE, VHEAD), 1.0, 6.0, ((0, 64), (1, 2)))
    lengths = uneven_parts(splits[14], SEQS, SEQS * CACHE // 2, CACHE, 2).astype(jnp.int32)
    mix_gain = jnp.clip(1.0 + 0.18 * jax.random.normal(splits[15], (D,), jnp.float32), 0.1, 1.9)
    expert_gate = gaussian(splits[16], (EXPERTS, D, FF), (D // 9) ** -0.5, 0.375, ((0, 64), (2, 2)))
    expert_up = gaussian(splits[17], (EXPERTS, D, FF), (D // 9) ** -0.5, 0.375, ((0, 64), (2, 2)))
    expert_down = gaussian(splits[18], (EXPERTS, FF, D), (9 * FF) ** -0.5, 0.0546875, ((0, 64), (1, 2)))
    routes_keys = jax.random.split(jax.random.fold_in(splits[19], 1), SEQS // SEQS_DEV)
    routes_turns = jax.random.permutation(jax.random.fold_in(splits[19], 3), SEQS // SEQS_DEV)
    routes = jax.vmap(lambda own, number: shared_out(jax.random.fold_in(splits[19], 2), own, number, SEQS_DEV, EXPERTS, TOP_K, CAP, 2))(routes_keys, routes_turns).reshape((SEQS, TOP_K))
    route_weight = jnp.clip(jnp.exp(math.log(0.59765625) - 2.4849066 * jax.random.uniform(splits[20], (SEQS, TOP_K), jnp.float32) ** level_of(splits[20], (SEQS, TOP_K), ((0, 64),), -0.2, 0.2)), 0.049804688, 0.59765625).astype(jnp.bfloat16)
    dense_mix = gaussian(splits[21], (D,), D ** -0.5, 0.125)
    dense_gate = gaussian(splits[22], (D, DENSE_FF), (D // 9) ** -0.5, 0.375, ((1, 128),))
    dense_up = gaussian(splits[23], (D, DENSE_FF), (D // 9) ** -0.5, 0.375, ((1, 128),))
    dense_down = gaussian(splits[24], (DENSE_FF, D), (9 * DENSE_FF) ** -0.5, 0.03125, ((0, 128),))
    return {"tokens": tokens, "attn_gain": attn_gain, "w_query1": w_query1, "w_query2": w_query2, "w_key1": w_key1, "w_key2": w_key2, "w_value": w_value, "query_gain": query_gain, "key_gain": key_gain, "head_lambda": head_lambda, "sub_gain": sub_gain, "w_output": w_output, "cache_key": cache_key, "cache_value": cache_value, "lengths": lengths, "mix_gain": mix_gain, "expert_gate": expert_gate, "expert_up": expert_up, "expert_down": expert_down, "routes": routes, "route_weight": route_weight, "dense_mix": dense_mix, "dense_gate": dense_gate, "dense_up": dense_up, "dense_down": dense_down}


epsilon = 1e-05
clamp_limit = 7.0
sigmoid_slope = 1.702
lambda_start = 0.2
neg_large = -1e+30

def rms_scale(values):
    return values * lax.rsqrt(lax.optimization_barrier(jnp.mean(values * values, axis=-1, keepdims=True)) + epsilon)

def clamped_unit(gate_pre, up_pre):
    gate_pre = jnp.minimum(gate_pre, clamp_limit)
    up_pre = jnp.clip(up_pre, -clamp_limit, clamp_limit)
    return gate_pre * jax.nn.sigmoid(sigmoid_slope * gate_pre) * (up_pre + 1.0)

def reference(tokens, attn_gain, w_query1, w_query2, w_key1, w_key2, w_value, query_gain, key_gain, head_lambda, sub_gain, w_output, cache_key, cache_value, lengths, mix_gain, expert_gate, expert_up, expert_down, routes, route_weight, dense_mix, dense_gate, dense_up, dense_down):
    groups = HEADS // KV_HEADS
    tokens_f = tokens.astype(jnp.float32)
    normed = (rms_scale(tokens_f) * attn_gain).astype(jnp.bfloat16)

    def project_query(weight):
        query = jnp.dot(normed, weight, preferred_element_type=jnp.float32)
        query = query.reshape(SEQS, KV_HEADS, groups, HEAD)
        return (rms_scale(query) * query_gain).astype(jnp.bfloat16)

    def project_key(weight):
        key_rows = jnp.dot(normed, weight, preferred_element_type=jnp.float32)
        key_rows = key_rows.reshape(SEQS, KV_HEADS, HEAD)
        return (rms_scale(key_rows) * key_gain).astype(jnp.bfloat16)
    first_query = project_query(w_query1)
    second_query = project_query(w_query2)
    first_key = project_key(w_key1)
    second_key = project_key(w_key2)
    new_value = jnp.dot(normed, w_value, preferred_element_type=jnp.float32).astype(jnp.bfloat16)
    new_value = new_value.reshape(SEQS, KV_HEADS, VHEAD)
    mixing = head_lambda.reshape(KV_HEADS, groups)
    scale = HEAD ** (-0.5)

    def one_sequence(inputs):
        query_a, query_b, key_a, key_b, value_new, keys_cached, values_cached, length = inputs
        valid = jnp.arange(CACHE, dtype=jnp.int32) < length

        def probs(query, cached_keys, fresh_key):
            query_f = query.astype(jnp.float32)
            cached = jnp.einsum('ghd,gpd->ghp', query_f, cached_keys.astype(jnp.float32)) * scale
            fresh = jnp.einsum('ghd,gd->gh', query_f, fresh_key.astype(jnp.float32)) * scale
            cached = jnp.where(valid[None, None, :], cached, neg_large)
            top = jnp.maximum(lax.optimization_barrier(jnp.max(cached, axis=-1)), fresh)
            cached_exp = jnp.exp(cached - top[..., None])
            fresh_exp = jnp.exp(fresh - top)
            total = lax.optimization_barrier(jnp.sum(cached_exp, axis=-1)) + fresh_exp
            return (cached_exp / total[..., None], fresh_exp / total)
        first_c, first_n = probs(query_a, keys_cached[..., :HEAD], key_a)
        second_c, second_n = probs(query_b, keys_cached[..., HEAD:], key_b)
        weight_c = (first_c - mixing[..., None] * second_c).astype(jnp.bfloat16)
        weight_n = (first_n - mixing * second_n).astype(jnp.bfloat16)
        out = jnp.einsum('ghp,gpe->ghe', weight_c.astype(jnp.float32), values_cached.astype(jnp.float32))
        return out + weight_n.astype(jnp.float32)[..., None] * value_new.astype(jnp.float32)[:, None, :]
    heads_out = lax.map(one_sequence, (first_query, second_query, first_key, second_key, new_value, cache_key, cache_value, lengths))
    sub_out = (rms_scale(heads_out) * sub_gain * (1.0 - lambda_start)).astype(jnp.bfloat16)
    sub_out = sub_out.reshape(SEQS, HEADS * VHEAD)
    per_half = HEADS * VHEAD // N_TP
    attn_out = jnp.zeros((SEQS, D), jnp.float32)
    for half in range(N_TP):
        partial_value = jnp.dot(sub_out[:, half * per_half:(half + 1) * per_half], w_output[half * per_half:(half + 1) * per_half], preferred_element_type=jnp.float32)
        attn_out = attn_out + lax.optimization_barrier(partial_value.astype(jnp.bfloat16)).astype(jnp.float32)
    residual = (tokens_f + attn_out).astype(jnp.bfloat16)
    mixed = (rms_scale(residual.astype(jnp.float32)) * mix_gain).astype(jnp.bfloat16)
    assign = routes.reshape(N_EP, SEQS_DEV * TOP_K)
    onehot = (assign[..., None] == jnp.arange(EXPERTS, dtype=jnp.int32)).astype(jnp.int32)
    ranks = lax.optimization_barrier(jnp.sum(onehot * (jnp.cumsum(onehot, axis=1) - onehot), axis=-1))
    rows_group = mixed.reshape(N_EP, SEQS_DEV, D).astype(jnp.float32)
    weights_group = route_weight.astype(jnp.float32).reshape(N_EP, SEQS_DEV, TOP_K)
    slot_ids = jnp.arange(CAP, dtype=jnp.int32)

    def per_expert(carry, inputs):
        gate_w, up_w, down_w, expert_id = inputs
        picked = (assign == expert_id)[:, None, :] & (ranks[:, None, :] == slot_ids[None, :, None])
        picked = picked.astype(jnp.float32).reshape(N_EP, CAP, SEQS_DEV, TOP_K)
        pick_rows = lax.optimization_barrier(jnp.sum(picked, axis=3))
        rows = jnp.einsum('bcs,bsd->bcd', pick_rows, rows_group).astype(jnp.bfloat16).reshape(N_EP * CAP, D)
        gate_pre = jnp.dot(rows, gate_w, preferred_element_type=jnp.float32)
        up_pre = jnp.dot(rows, up_w, preferred_element_type=jnp.float32)
        hidden = clamped_unit(gate_pre, up_pre).astype(jnp.bfloat16)
        out = jnp.dot(hidden, down_w, preferred_element_type=jnp.float32).astype(jnp.bfloat16)
        out = out.reshape(N_EP, CAP, D).astype(jnp.float32)
        weighted = lax.optimization_barrier(jnp.sum(picked * weights_group[:, None], axis=3))
        return (carry + jnp.einsum('bcs,bcd->bsd', weighted, out, precision=lax.Precision.HIGHEST), None)
    routed, _ = lax.scan(per_expert, jnp.zeros((N_EP, SEQS_DEV, D), jnp.float32), (expert_gate, expert_up, expert_down, jnp.arange(EXPERTS, dtype=jnp.int32)))
    routed = routed.reshape(SEQS, D)
    dense_hidden = clamped_unit(jnp.dot(mixed, dense_gate, preferred_element_type=jnp.float32), jnp.dot(mixed, dense_up, preferred_element_type=jnp.float32)).astype(jnp.bfloat16)
    dense = jnp.dot(dense_hidden, dense_down, preferred_element_type=jnp.float32)
    row_gate = jax.nn.sigmoid(jnp.dot(mixed, dense_mix, preferred_element_type=jnp.float32))
    total = residual.astype(jnp.float32) + routed + row_gate[:, None] * dense
    return total.astype(jnp.bfloat16)
```

```python
import functools

import jax
import jax.numpy as jnp
from jax import lax
from jax.experimental import pallas as pl
from jax.experimental.pallas import tpu as pltpu
from jax.sharding import Mesh
from jax.sharding import PartitionSpec as P

HEAD = 64
VHEAD = 128
EP = ("ep_0", "ep_1", "ep_2")
EP_TP = ("ep_0", "ep_1", "ep_2", "tp")
SLOTS = 8
CAP = 2
DENSE_ROWS = 4
SEQ_STEP = 4
FF_TILE = 256

epsilon = 1e-05
clamp_limit = 7.0
sigmoid_slope = 1.702
lambda_start = 0.2
neg_large = -1e30

bf16 = jnp.bfloat16
f32 = jnp.float32
NT = (((1,), (1,)), ((), ()))
TN = (((0,), (0,)), ((), ()))


def mm(a, b, dims=(((1,), (0,)), ((), ()))):
    return lax.dot_general(a, b, dims, preferred_element_type=f32)


def clamped_unit(gate_pre, up_pre):
    gate_pre = jnp.minimum(gate_pre, clamp_limit)
    up_pre = jnp.clip(up_pre, -clamp_limit, clamp_limit)
    return gate_pre * jax.nn.sigmoid(sigmoid_slope * gate_pre) * (up_pre + 1.0)


def rms(values):
    return lax.rsqrt(jnp.mean(values * values, axis=-1, keepdims=True) + epsilon)


def routing_maps(routes_t, weight_t, seqs, peers):
    wide = peers * SLOTS
    diag = lax.broadcasted_iota(jnp.int32, (seqs, seqs), 0) == lax.broadcasted_iota(
        jnp.int32, (seqs, seqs), 1
    )
    lane = lax.broadcasted_iota(jnp.int32, (seqs, wide), 1)
    peer, slot = lane // SLOTS, lane % SLOTS
    token = lax.broadcasted_iota(jnp.int32, (seqs, wide), 0)
    hit = jnp.zeros((seqs, wide), f32)
    weight = jnp.zeros((seqs, wide), f32)
    for k in range(routes_t.shape[0]):
        expert = jnp.sum(
            jnp.where(diag, routes_t[k : k + 1, :].astype(f32), 0.0), axis=1, keepdims=True
        ).astype(jnp.int32)
        share = jnp.sum(
            jnp.where(diag, weight_t[k : k + 1, :].astype(f32), 0.0), axis=1, keepdims=True
        )
        same = peer == expert
        hit = jnp.where(same, 1.0, hit)
        weight = jnp.where(same, share, weight)
    before = (
        lax.broadcasted_iota(jnp.int32, (seqs, seqs), 1)
        < lax.broadcasted_iota(jnp.int32, (seqs, seqs), 0)
    ).astype(bf16)
    rank = mm(before, hit.astype(bf16))
    chosen = (hit > 0.0) & (rank == slot.astype(f32)) & (slot < CAP)
    group = 2 * ((peer // 16) % 2) + (peer // 4) % 2
    dense = (token == group * DENSE_ROWS + slot - CAP) & (slot >= CAP) & (slot < CAP + DENSE_ROWS)
    send = jnp.where(chosen | dense, 1.0, 0.0).astype(bf16)
    return (
        send,
        jnp.where(chosen, weight, 0.0).astype(bf16),
        jnp.where(dense, 1.0, 0.0).astype(bf16),
    )


def attention_kernel(
    lengths,
    lam,
    tokens,
    attn_gain,
    w_query1,
    w_query2,
    w_key1,
    w_key2,
    w_value,
    query_gain,
    key_gain,
    sub_gain,
    routes_t,
    weight_t,
    w_output,
    cache_key,
    cache_value,
    out,
    send_map,
    home_map,
    query_s,
    key_s,
    value_s,
    heads_s,
    output_s,
    sem,
    *,
    peers,
):
    step = pl.program_id(0)
    seqs = tokens.shape[0]
    heads = w_query1.shape[1] // HEAD
    fetch = pltpu.make_async_copy(w_output, output_s, sem)

    @pl.when(step == 0)
    def _():
        fetch.start()
        rows = tokens[...].astype(f32)
        normed = (rows * rms(rows) * attn_gain[...]).astype(bf16)
        nothing = jnp.zeros((seqs, HEAD), f32)
        for m, weight in enumerate((w_query1, w_query2)):
            query = mm(normed, weight[...])
            for h in range(heads):
                one = query[:, h * HEAD : (h + 1) * HEAD]
                one = (one * rms(one) * query_gain[...]).astype(bf16).astype(f32) * HEAD**-0.5
                pair = (one, nothing) if m == 0 else (nothing, one)
                at = (m * heads + h) * seqs
                query_s[at : at + seqs, :] = jnp.concatenate(pair, axis=1)
        keys = []
        for weight in (w_key1, w_key2):
            one = mm(normed, weight[...], NT)
            keys.append((one * rms(one) * key_gain[...]).astype(bf16).astype(f32))
        key_s[...] = jnp.concatenate(keys, axis=1)
        value_s[...] = mm(normed, w_value[...]).astype(bf16).astype(f32)
        send, routed, dense = routing_maps(routes_t[...], weight_t[...], seqs, peers)
        send_map[...] = send
        home_map[0:seqs, :] = routed
        home_map[seqs : 2 * seqs, :] = dense

    cached = cache_key.shape[2]
    row = lax.broadcasted_iota(jnp.int32, (2 * heads, 1), 0)
    signed = jnp.ones((2 * heads, 1), f32)
    for h in range(heads):
        signed = jnp.where(row == heads + h, -lam[h], signed)
    lane = lax.broadcasted_iota(jnp.int32, (2 * heads, cached), 1)
    for i in range(cache_key.shape[0]):
        s = step * cache_key.shape[0] + i
        query = query_s[pl.ds(s, 2 * heads, stride=seqs), :]
        fresh = jnp.sum(query * key_s[pl.ds(s, 1), :], axis=1, keepdims=True)
        scores = mm(query.astype(bf16), cache_key[i, 0], NT)
        scores = jnp.where(lane < lengths[s], scores, neg_large)
        top = jnp.maximum(jnp.max(scores, axis=1, keepdims=True), fresh)
        expo = jnp.exp(scores - top)
        fresh_expo = jnp.exp(fresh - top)
        scale = signed / (jnp.sum(expo, axis=1, keepdims=True) + fresh_expo)
        probs = expo * scale
        probs = (probs + pltpu.roll(probs, heads, 0)).astype(bf16)
        fresh_probs = fresh_expo * scale
        fresh_probs = fresh_probs[0:heads] + fresh_probs[heads:]
        heads_out = mm(probs, cache_value[i, 0])[0:heads]
        heads_out = heads_out + fresh_probs.astype(bf16).astype(f32) * value_s[pl.ds(s, 1), :]
        heads_s[pl.ds(s, heads, stride=seqs), :] = heads_out

    @pl.when(step == pl.num_programs(0) - 1)
    def _():
        subs = []
        for h in range(heads):
            one = heads_s[h * seqs : (h + 1) * seqs, :]
            subs.append((one * rms(one) * sub_gain[...] * (1.0 - lambda_start)).astype(bf16))
        fetch.wait()
        out[...] = mm(jnp.concatenate(subs, axis=1), output_s[...]).astype(bf16)


def attention(
    tokens, attn_gain, w_query1, w_query2, w_key1, w_key2, w_value, query_gain, key_gain,
    head_lambda, sub_gain, w_output, cache_key, cache_value, lengths, routes, route_weight, peers,
):
    seqs, width = tokens.shape
    heads = w_query1.shape[1] // HEAD
    cached = cache_key.shape[2]
    whole = pl.BlockSpec(memory_space=pltpu.VMEM)
    smem = pl.BlockSpec(memory_space=pltpu.SMEM)
    cache_spec = pl.BlockSpec((SEQ_STEP, 1, cached, VHEAD), lambda i: (i, 0, 0, 0))
    flops = 2 * seqs * width * (2 * heads * HEAD + 2 * HEAD + VHEAD + heads * VHEAD)
    flops += 6 * seqs * 8 * cached * VHEAD
    wide = peers * SLOTS
    return pl.pallas_call(
        functools.partial(attention_kernel, peers=peers),
        grid=(seqs // SEQ_STEP,),
        in_specs=[smem, smem] + [whole] * 12
        + [pl.BlockSpec(memory_space=pl.ANY), cache_spec, cache_spec],
        out_specs=[whole] * 3,
        out_shape=[
            jax.ShapeDtypeStruct((seqs, width), bf16),
            jax.ShapeDtypeStruct((seqs, wide), bf16),
            jax.ShapeDtypeStruct((2 * seqs, wide), bf16),
        ],
        scratch_shapes=[
            pltpu.VMEM((2 * heads * seqs, 2 * HEAD), f32),
            pltpu.VMEM((seqs, 2 * HEAD), f32),
            pltpu.VMEM((seqs, VHEAD), f32),
            pltpu.VMEM((heads * seqs, VHEAD), f32),
            pltpu.VMEM(w_output.shape, bf16),
            pltpu.SemaphoreType.DMA,
        ],
        compiler_params=pltpu.CompilerParams(vmem_limit_bytes=32 << 20),
        cost_estimate=pl.CostEstimate(
            flops=flops, bytes_accessed=13 << 20, transcendentals=seqs * 8 * cached
        ),
        name="attention",
    )(
        lengths, head_lambda, tokens, attn_gain.reshape(1, -1), w_query1, w_query2, w_key1.T,
        w_key2.T, w_value, query_gain.reshape(1, -1), key_gain.reshape(1, -1),
        sub_gain.reshape(1, -1), routes.T, route_weight.T, w_output, cache_key, cache_value,
    )


def mix_kernel(core, tokens, mine, other, mix_gain, dense_mix, send_map, send, kept, row_gate):
    half = send.shape[1]
    attn_out = mine[...].astype(f32) + other[...].astype(f32)
    residual = (tokens[...].astype(f32) + attn_out).astype(bf16)
    rows = residual.astype(f32)
    mixed = (rows * rms(rows) * mix_gain[...]).astype(bf16)
    first = core[0] == 0
    kept[...] = jnp.where(first, rows[:, :half], rows[:, half:])
    gate = jnp.sum(mixed.astype(f32) * dense_mix[...].astype(f32), axis=1, keepdims=True)
    row_gate[...] = jnp.broadcast_to(jax.nn.sigmoid(gate), row_gate.shape)
    mixed = mixed.astype(f32)
    columns = jnp.where(first, mixed[:, :half], mixed[:, half:]).astype(bf16)
    send[...] = mm(send_map[...], columns, TN).astype(bf16)


def mix(core, tokens, mine, other, mix_gain, dense_mix, send_map):
    seqs, width = tokens.shape
    wide, half = send_map.shape[1], width // 2
    whole = pl.BlockSpec(memory_space=pltpu.VMEM)
    return pl.pallas_call(
        mix_kernel,
        in_specs=[pl.BlockSpec(memory_space=pltpu.SMEM)] + [whole] * 6,
        out_specs=[whole] * 3,
        out_shape=[
            jax.ShapeDtypeStruct((wide, half), bf16),
            jax.ShapeDtypeStruct((seqs, half), f32),
            jax.ShapeDtypeStruct((seqs, 128), f32),
        ],
        compiler_params=pltpu.CompilerParams(vmem_limit_bytes=32 << 20),
        cost_estimate=pl.CostEstimate(
            flops=2 * wide * seqs * half, bytes_accessed=2 << 20, transcendentals=0
        ),
        name="mix",
    )(core, tokens, mine, other, mix_gain.reshape(1, -1), dense_mix.reshape(1, -1), send_map)


def expert_kernel(core, mine, other, gate, up, down, out_mine, out_other, rows_s, total):
    step = pl.program_id(0)
    half = mine.shape[1]
    slots = rows_s.shape[0]

    @pl.when(step == 0)
    def _():
        wide = mine.shape[0]
        row = lax.broadcasted_iota(jnp.int32, (slots, wide), 0)
        lane = lax.broadcasted_iota(jnp.int32, (slots, wide), 1)
        pick = jnp.where(lane == (row // CAP) * SLOTS + row % CAP, 1.0, 0.0).astype(bf16)
        at = pl.multiple_of(core[0] * half, half)
        rows_s[:, pl.ds(at, half)] = mm(pick, mine[...]).astype(bf16)
        at = pl.multiple_of((1 - core[0]) * half, half)
        rows_s[:, pl.ds(at, half)] = mm(pick, other[...]).astype(bf16)

    rows = rows_s[...]
    hidden = clamped_unit(mm(rows, gate[0]), mm(rows, up[0])).astype(bf16)
    part = mm(hidden, down[0])

    @pl.when(step == 0)
    def _():
        total[...] = part

    @pl.when(step > 0)
    def _():
        total[...] += part

    @pl.when(step == pl.num_programs(0) - 1)
    def _():
        at = pl.multiple_of(core[0] * half, half)
        out_mine[...] = total[:, pl.ds(at, half)].astype(bf16)
        at = pl.multiple_of((1 - core[0]) * half, half)
        out_other[...] = total[:, pl.ds(at, half)].astype(bf16)


def experts(core, mine, other, gate, up, down):
    wide, half = mine.shape
    _, width, hidden = gate.shape
    slots = wide // SLOTS * CAP
    whole = pl.BlockSpec(memory_space=pltpu.VMEM)
    return pl.pallas_call(
        expert_kernel,
        grid=(hidden // FF_TILE,),
        in_specs=[
            pl.BlockSpec(memory_space=pltpu.SMEM),
            whole,
            whole,
            pl.BlockSpec((1, width, FF_TILE), lambda i: (0, 0, i)),
            pl.BlockSpec((1, width, FF_TILE), lambda i: (0, 0, i)),
            pl.BlockSpec((1, FF_TILE, width), lambda i: (0, i, 0)),
        ],
        out_specs=[whole, whole],
        out_shape=[jax.ShapeDtypeStruct((slots, half), bf16)] * 2,
        scratch_shapes=[pltpu.VMEM((slots, width), bf16), pltpu.VMEM((slots, width), f32)],
        compiler_params=pltpu.CompilerParams(vmem_limit_bytes=32 << 20),
        cost_estimate=pl.CostEstimate(
            flops=6 * slots * width * hidden,
            bytes_accessed=6 * width * hidden + 4 * wide * half,
            transcendentals=slots * hidden,
        ),
        name="experts",
    )(core, mine, other, gate, up, down)


def dense_kernel(core, mine, other, *refs):
    packs, out, gate_s, up_s, down_s = refs[:-4], refs[-4], refs[-3], refs[-2], refs[-1]
    half = mine.shape[1]
    units = packs[0].shape[0] // 3
    at = pl.multiple_of(core[0] * half, half)
    back = pl.multiple_of((1 - core[0]) * half, half)
    for i, pack in enumerate(packs):
        to = slice(i * units, (i + 1) * units)
        gate_s[to, :] = pack[0:units, :]
        up_s[to, :] = pack[units : 2 * units, :]
        down_s[to, :] = pack[2 * units : 3 * units, pl.ds(at, half)]
    rows, far = mine[...], other[...]
    gate = mm(rows, gate_s[:, pl.ds(at, half)], NT) + mm(far, gate_s[:, pl.ds(back, half)], NT)
    up = mm(rows, up_s[:, pl.ds(at, half)], NT) + mm(far, up_s[:, pl.ds(back, half)], NT)
    slot = lax.broadcasted_iota(jnp.int32, gate.shape, 0) % SLOTS
    used = (slot >= CAP) & (slot < CAP + DENSE_ROWS)
    hidden = jnp.where(used, clamped_unit(gate, up), 0.0).astype(bf16)
    out[...] = mm(hidden, down_s[...]).astype(bf16)


def dense_part(core, mine, other, packs):
    wide, half = mine.shape
    units = packs[0].shape[0] // 3
    many = units * len(packs)
    whole = pl.BlockSpec(memory_space=pltpu.VMEM)
    return pl.pallas_call(
        dense_kernel,
        in_specs=[pl.BlockSpec(memory_space=pltpu.SMEM)] + [whole] * (2 + len(packs)),
        out_specs=whole,
        out_shape=jax.ShapeDtypeStruct((wide, half), bf16),
        scratch_shapes=[
            pltpu.VMEM((many, 2 * half), bf16),
            pltpu.VMEM((many, 2 * half), bf16),
            pltpu.VMEM((many, half), bf16),
        ],
        compiler_params=pltpu.CompilerParams(vmem_limit_bytes=32 << 20),
        cost_estimate=pl.CostEstimate(
            flops=10 * wide * half * many, bytes_accessed=6 << 20, transcendentals=wide * many
        ),
        name="dense",
    )(core, mine, other, *packs)


def join_kernel(dense, mine, other, out):
    total = (mine[...].astype(f32) + other[...].astype(f32)).astype(bf16)
    wide, slots = dense.shape[0], total.shape[0]
    row = lax.broadcasted_iota(jnp.int32, (wide, slots), 0)
    lane = lax.broadcasted_iota(jnp.int32, (wide, slots), 1)
    spread = jnp.where(row == (lane // CAP) * SLOTS + lane % CAP, 1.0, 0.0).astype(bf16)
    out[...] = (dense[...].astype(f32) + mm(spread, total)).astype(bf16)


def join(dense, mine, other):
    whole = pl.BlockSpec(memory_space=pltpu.VMEM)
    return pl.pallas_call(
        join_kernel,
        in_specs=[whole] * 3,
        out_specs=whole,
        out_shape=jax.ShapeDtypeStruct(dense.shape, bf16),
        compiler_params=pltpu.CompilerParams(vmem_limit_bytes=32 << 20),
        cost_estimate=pl.CostEstimate(
            flops=2 * dense.size * mine.shape[0], bytes_accessed=3 << 20, transcendentals=0
        ),
        name="join",
    )(dense, mine, other)


def home_kernel(home_map, returned, kept, row_gate, out):
    seqs = kept.shape[0]
    sums = mm(home_map[...], returned[...])
    out[...] = (kept[...] + sums[:seqs] + row_gate[:, 0:1] * sums[seqs:]).astype(bf16)


def home(home_map, returned, kept, row_gate):
    whole = pl.BlockSpec(memory_space=pltpu.VMEM)
    return pl.pallas_call(
        home_kernel,
        in_specs=[whole] * 4,
        out_specs=whole,
        out_shape=jax.ShapeDtypeStruct(kept.shape, bf16),
        compiler_params=pltpu.CompilerParams(vmem_limit_bytes=32 << 20),
        cost_estimate=pl.CostEstimate(
            flops=2 * home_map.shape[0] * returned.size, bytes_accessed=1 << 20, transcendentals=0
        ),
        name="home",
    )(home_map, returned, kept, row_gate)


def swap(array):
    return lax.ppermute(array, "tp", [(0, 1), (1, 0)])


def from_square(array):
    got = []
    for flip0, flip1 in ((1, 0), (0, 1), (1, 1)):
        pairs = [(4 * a + b, 4 * (a ^ flip0) + (b ^ flip1)) for a in range(4) for b in range(4)]
        got.append(lax.ppermute(array, ("ep_0", "ep_1"), pairs))
    return got


def shards(
    tokens, attn_gain, w_query1, w_query2, w_key1, w_key2, w_value, query_gain, key_gain,
    head_lambda, sub_gain, w_output, cache_key, cache_value, lengths, mix_gain, expert_gate,
    expert_up, expert_down, routes, route_weight, dense_mix, dense_gate, dense_up, dense_down,
):
    peers = lax.axis_size(EP)
    core = lax.axis_index("tp").astype(jnp.int32).reshape(1)
    pack = jnp.concatenate([dense_gate.T, dense_up.T, dense_down], axis=0)
    packs = [pack] + from_square(pack)
    part, send_map, home_map = attention(
        tokens, attn_gain, w_query1, w_query2, w_key1, w_key2, w_value, query_gain, key_gain,
        head_lambda, sub_gain, w_output, cache_key, cache_value, lengths, routes, route_weight,
        peers,
    )
    send, kept, row_gate = mix(core, tokens, part, swap(part), mix_gain, dense_mix, send_map)
    wide, half = send.shape

    def exchange(blocks):
        blocks = blocks.reshape(peers, SLOTS, half)
        return lax.all_to_all(blocks, EP, 0, 0, tiled=True).reshape(wide, half)

    mine = exchange(send)
    other = swap(mine)
    own, sent = experts(core, mine, other, expert_gate, expert_up, expert_down)
    came = swap(sent)
    packs = packs + [swap(one) for one in packs]
    dense = dense_part(core, mine, other, packs)
    returned = exchange(join(dense, own, came))
    return home(home_map, returned, kept, row_gate)


def solution(mesh):
    torus = Mesh(mesh.devices.reshape(4, 4, 4, mesh.shape["tp"]), EP_TP)
    in_specs = (
        P(EP, None), P(), P(None, "tp"), P(None, "tp"), P(None, "tp"), P(None, "tp"),
        P(None, "tp"), P(), P(), P("tp"), P(), P("tp", None), P(EP, "tp", None, None),
        P(EP, "tp", None, None), P(EP), P(), P(EP, None, "tp"), P(EP, None, "tp"),
        P(EP, "tp", None), P(EP, None), P(EP, None), P(), P(None, EP_TP), P(None, EP_TP),
        P(EP_TP, None),
    )
    return jax.shard_map(
        shards, mesh=torus, in_specs=in_specs, out_specs=P(EP, "tp"), check_vma=False
    )
```

```python
import functools

import jax
import jax.numpy as jnp
from jax import lax
from jax.experimental import pallas as pl
from jax.experimental.pallas import tpu as pltpu
from jax.sharding import Mesh
from jax.sharding import PartitionSpec as P


HEAD = 64
VHEAD = 128
EP = ("ep_0", "ep_1", "ep_2")
EP_TP = ("ep_0", "ep_1", "ep_2", "tp")
SLOTS = 6
CAP = 2
DENSE_ROWS = 4
LANES = 128
SEQ_STEP = 4
LIMIT = 40 << 20

epsilon = 1e-05
clamp_limit = 7.0
sigmoid_slope = 1.702
lambda_start = 0.2
neg_large = -1e30

bf16 = jnp.bfloat16
f32 = jnp.float32
NT = (((1,), (1,)), ((), ()))
TN = (((0,), (0,)), ((), ()))


def mm(a, b, dims=(((1,), (0,)), ((), ()))):
    return lax.dot_general(a, b, dims, preferred_element_type=f32)


def clamped_unit(gate_pre, up_pre):
    gate_pre = jnp.minimum(gate_pre, clamp_limit)
    up_pre = jnp.clip(up_pre, -clamp_limit, clamp_limit)
    return gate_pre * jax.nn.sigmoid(sigmoid_slope * gate_pre) * (up_pre + 1.0)


def rms(values):
    return lax.rsqrt(jnp.mean(values * values, axis=-1, keepdims=True) + epsilon)


def routing_maps(routes_t, weight_t, seqs, peers):
    wide = peers * SLOTS
    diag = lax.broadcasted_iota(jnp.int32, (seqs, seqs), 0) == lax.broadcasted_iota(
        jnp.int32, (seqs, seqs), 1
    )
    lane = lax.broadcasted_iota(jnp.int32, (seqs, wide), 1)
    peer, slot = lane % peers, lane // peers
    token = lax.broadcasted_iota(jnp.int32, (seqs, wide), 0)
    hit = jnp.zeros((seqs, wide), f32)
    weight = jnp.zeros((seqs, wide), f32)
    for k in range(routes_t.shape[0]):
        expert = jnp.sum(
            jnp.where(diag, routes_t[k : k + 1, :].astype(f32), 0.0), axis=1, keepdims=True
        ).astype(jnp.int32)
        share = jnp.sum(
            jnp.where(diag, weight_t[k : k + 1, :].astype(f32), 0.0), axis=1, keepdims=True
        )
        same = peer == expert
        hit = jnp.where(same, 1.0, hit)
        weight = jnp.where(same, share, weight)
    before = (
        lax.broadcasted_iota(jnp.int32, (seqs, seqs), 1)
        < lax.broadcasted_iota(jnp.int32, (seqs, seqs), 0)
    ).astype(bf16)
    rank = mm(before, hit.astype(bf16))
    chosen = (hit > 0.0) & (rank == slot.astype(f32)) & (slot < CAP)
    group = 2 * ((peer // 16) % 2) + (peer // 4) % 2
    dense = (token == group * DENSE_ROWS + slot - CAP) & (slot >= CAP)
    return (
        jnp.where(chosen | dense, 1.0, 0.0).astype(bf16),
        jnp.where(chosen, weight, 0.0).astype(bf16),
        jnp.where(dense, 1.0, 0.0).astype(bf16),
    )


def attention_kernel(*refs, peers):
    sources, refs = refs[:17], refs[17:]
    part, send_map, home_map = refs[:3]
    query_s, key_s, value_s, heads_s, *local = refs[3:-1]
    sems = refs[-1]
    (
        lengths, lam, tokens, attn_gain, w_query1, w_query2, w_key1, w_key2, w_value, query_gain, key_gain,
        routes_t, weight_t, sub_gain, w_output, cache_key, cache_value,
    ) = local
    seqs = tokens.shape[0]
    heads = w_query1.shape[1] // HEAD
    cached = cache_key.shape[2]
    rounds = seqs // SEQ_STEP
    copies = [
        pltpu.make_async_copy(sources[i], local[i], sems.at[i]) for i in range(len(local) - 2)
    ]
    chunks = []
    for b in range(rounds):
        of = pl.ds(b * SEQ_STEP, SEQ_STEP)
        for j in (0, 1):
            at = len(copies) + len(chunks)
            source, to = sources[15 + j].at[of], local[15 + j].at[of]
            chunks.append(pltpu.make_async_copy(source, to, sems.at[at]))
    for one in copies[:-1] + chunks + copies[-1:]:
        one.start()

    for one in copies[:-1]:
        one.wait()
    rows = tokens[...].astype(f32)
    normed = (rows * rms(rows) * attn_gain[...]).astype(bf16)
    nothing = jnp.zeros((seqs, HEAD), f32)
    for m, weight in enumerate((w_query1, w_query2)):
        query = mm(normed, weight[...])
        for h in range(heads):
            one = query[:, h * HEAD : (h + 1) * HEAD]
            one = (one * rms(one) * query_gain[...]).astype(bf16).astype(f32) * HEAD**-0.5
            pair = (one, nothing) if m == 0 else (nothing, one)
            at = (m * heads + h) * seqs
            query_s[at : at + seqs, :] = jnp.concatenate(pair, axis=1)
    new_keys = []
    for weight in (w_key1, w_key2):
        one = mm(normed, weight[...], NT)
        new_keys.append((one * rms(one) * key_gain[...]).astype(bf16).astype(f32))
    key_s[...] = jnp.concatenate(new_keys, axis=1)
    value_s[...] = mm(normed, w_value[...]).astype(bf16).astype(f32)
    send, routed, dense = routing_maps(routes_t[...], weight_t[...], seqs, peers)
    send_map[...] = send
    home_map[0:seqs, :] = routed
    home_map[seqs : 2 * seqs, :] = dense

    row = lax.broadcasted_iota(jnp.int32, (2 * heads, 1), 0)
    signed = jnp.ones((2 * heads, 1), f32)
    for h in range(heads):
        signed = jnp.where(row == heads + h, -lam[h], signed)
    lane = lax.broadcasted_iota(jnp.int32, (2 * heads, cached), 1)
    for b in range(rounds):
        chunks[2 * b].wait()
        chunks[2 * b + 1].wait()
        for s in range(b * SEQ_STEP, (b + 1) * SEQ_STEP):
            query = query_s[pl.ds(s, 2 * heads, stride=seqs), :]
            fresh = jnp.sum(query * key_s[s : s + 1, :], axis=1, keepdims=True)
            scores = mm(query.astype(bf16), cache_key[s, 0], NT)
            scores = jnp.where(lane < lengths[s], scores, neg_large)
            top = jnp.maximum(jnp.max(scores, axis=1, keepdims=True), fresh)
            expo = jnp.exp(scores - top)
            fresh_expo = jnp.exp(fresh - top)
            scale = signed / (jnp.sum(expo, axis=1, keepdims=True) + fresh_expo)
            probs = expo * scale
            probs = (probs + pltpu.roll(probs, heads, 0)).astype(bf16)
            fresh_probs = fresh_expo * scale
            fresh_probs = fresh_probs[0:heads] + fresh_probs[heads:]
            heads_out = mm(probs, cache_value[s, 0])[0:heads]
            heads_out = heads_out + fresh_probs.astype(bf16).astype(f32) * value_s[s : s + 1, :]
            heads_s[pl.ds(s, heads, stride=seqs), :] = heads_out

    subs = []
    for h in range(heads):
        one = heads_s[h * seqs : (h + 1) * seqs, :]
        subs.append((one * rms(one) * sub_gain[...] * (1.0 - lambda_start)).astype(bf16))
    copies[-1].wait()
    part[...] = mm(jnp.concatenate(subs, axis=1), w_output[...]).astype(bf16)


def attention(
    tokens, attn_gain, w_query1, w_query2, w_key1, w_key2, w_value, query_gain, key_gain,
    head_lambda, sub_gain, w_output, cache_key, cache_value, lengths, routes, route_weight,
    peers,
):
    seqs, width = tokens.shape
    heads = w_query1.shape[1] // HEAD
    cached = cache_key.shape[2]
    local = [
        lengths, head_lambda, tokens, attn_gain.reshape(1, -1), w_query1, w_query2, w_key1.T, w_key2.T, w_value,
        query_gain.reshape(1, -1), key_gain.reshape(1, -1), routes.T, route_weight.T,
        sub_gain.reshape(1, -1), w_output, cache_key, cache_value,
    ]
    flops = 2 * seqs * width * (2 * heads * HEAD + 2 * HEAD + VHEAD + heads * VHEAD)
    flops += 6 * seqs * 8 * cached * VHEAD
    wide = peers * SLOTS
    count = len(local) - 2 + 2 * (seqs // SEQ_STEP)
    return pl.pallas_call(
        functools.partial(attention_kernel, peers=peers),
        in_specs=[pl.BlockSpec(memory_space=pltpu.HBM)] * len(local),
        out_specs=[pl.BlockSpec(memory_space=pltpu.VMEM)] * 3,
        out_shape=[
            pltpu.VMEM((seqs, width), bf16),
            pltpu.VMEM((seqs, wide), bf16),
            pltpu.VMEM((2 * seqs, wide), bf16),
        ],
        scratch_shapes=[
            pltpu.VMEM((2 * heads * seqs, 2 * HEAD), f32),
            pltpu.VMEM((seqs, 2 * HEAD), f32),
            pltpu.VMEM((seqs, VHEAD), f32),
            pltpu.VMEM((heads * seqs, VHEAD), f32),
        ]
        + [pltpu.SMEM(one.shape, one.dtype) for one in local[:2]]
        + [pltpu.VMEM(one.shape, one.dtype) for one in local[2:]]
        + [pltpu.SemaphoreType.DMA((count,))],
        compiler_params=pltpu.CompilerParams(vmem_limit_bytes=LIMIT),
        cost_estimate=pl.CostEstimate(
            flops=flops, bytes_accessed=13 << 20, transcendentals=seqs * 8 * cached
        ),
        name="attention",
    )(*[pltpu.with_memory_space_constraint(one, pltpu.HBM) for one in local])


def spread(wide_s, rows, first):
    slots, peers, parts = wide_s.shape[0] // 64 // 8, 64, rows.shape[1] // LANES
    for r in range(rows.shape[0] // peers):
        for c in range(parts):
            wide_s[pl.ds((first + r) * parts + c, peers, stride=slots * parts), :] = rows[
                r * peers : (r + 1) * peers, c * LANES : (c + 1) * LANES
            ]


def gather(wide_s, r, c, parts, peers):
    slots = wide_s.shape[0] // peers // parts
    return wide_s[pl.ds(r * parts + c, peers, stride=slots * parts), :].astype(bf16)


def mix_kernel(core, tokens, mine, other, mix_gain, dense_mix, send_map, send, kept, row_gate, wide_s):
    half = kept.shape[1]
    attn_out = mine[...].astype(f32) + other[...].astype(f32)
    residual = (tokens[...].astype(f32) + attn_out).astype(bf16)
    rows = residual.astype(f32)
    mixed = (rows * rms(rows) * mix_gain[...]).astype(bf16).astype(f32)
    first = core[0] == 0
    kept[...] = jnp.where(first, rows[:, :half], rows[:, half:])
    gate = jnp.zeros((rows.shape[0], LANES), f32)
    for c in range(rows.shape[1] // LANES):
        gate = gate + mixed[:, c * LANES : (c + 1) * LANES] * dense_mix[c : c + 1, :].astype(f32)
    gate = jnp.sum(gate, axis=1, keepdims=True)
    row_gate[...] = jnp.broadcast_to(jax.nn.sigmoid(gate), row_gate.shape)
    columns = jnp.where(first, mixed[:, :half], mixed[:, half:]).astype(bf16)
    spread(wide_s, mm(send_map[...], columns, TN), 0)
    send[...] = wide_s[...].astype(bf16)


def call(kernel, args, outs, scratch, flops, transcendentals=0, far=0):
    near = len(args) - far
    spaces = [pltpu.SMEM if one.ndim == 1 else pltpu.VMEM for one in args[:near]]
    spaces += [pltpu.HBM] * far
    args = list(args[:near]) + [
        pltpu.with_memory_space_constraint(one, pltpu.HBM) for one in args[near:]
    ]
    out_shape = [jax.ShapeDtypeStruct(*one) for one in outs]
    moved = sum(one.size * one.dtype.itemsize for one in args + out_shape)
    return pl.pallas_call(
        kernel,
        in_specs=[pl.BlockSpec(memory_space=space) for space in spaces],
        out_specs=[pl.BlockSpec(memory_space=pltpu.VMEM)] * len(outs),
        out_shape=out_shape,
        scratch_shapes=[pltpu.VMEM(*one) for one in scratch]
        + [pltpu.SemaphoreType.DMA((far,))] * (far > 0),
        compiler_params=pltpu.CompilerParams(vmem_limit_bytes=LIMIT // 2),
        cost_estimate=pl.CostEstimate(
            flops=flops, bytes_accessed=moved, transcendentals=transcendentals
        ),
    )(*args)


def compact(wide_s, rows_e, rows_d):
    parts, peers = rows_d.shape[1] // LANES, rows_e.shape[0] // CAP
    for r in range(SLOTS):
        for c in range(parts):
            to, at = (rows_e, r) if r < CAP else (rows_d, r - CAP)
            to[at * peers : (at + 1) * peers, c * LANES : (c + 1) * LANES] = gather(
                wide_s, r, c, parts, peers
            )


def first_kernel(
    core, mine, gate_far, up_far, rows_d, gate_part, up_part, wide_s, rows_e, gate, up, sems
):
    half = rows_d.shape[1]
    own = pl.ds(pl.multiple_of(core[0] * half, half), half)
    fetch_gate = pltpu.make_async_copy(gate_far.at[0, own], gate, sems.at[0])
    fetch_up = pltpu.make_async_copy(up_far.at[0, own], up, sems.at[1])
    fetch_gate.start()
    fetch_up.start()
    wide_s[...] = mine[...].astype(f32)
    compact(wide_s, rows_e, rows_d)
    fetch_gate.wait()
    gate_part[...] = mm(rows_e[...], gate[...])
    fetch_up.wait()
    up_part[...] = mm(rows_e[...], up[...])


def second_kernel(
    core, other, gate_part, up_part, gate_far, up_far, down_far, rows_d, out_mine, out_other,
    wide_s, rows_e, total, gate, up, down, sems,
):
    half = rows_d.shape[1]
    at = pl.multiple_of(core[0] * half, half)
    back = pl.multiple_of((1 - core[0]) * half, half)
    fetch_gate = pltpu.make_async_copy(gate_far.at[0, pl.ds(back, half)], gate, sems.at[0])
    fetch_up = pltpu.make_async_copy(up_far.at[0, pl.ds(back, half)], up, sems.at[1])
    fetch_down = pltpu.make_async_copy(down_far.at[0], down, sems.at[2])
    fetch_gate.start()
    fetch_up.start()
    fetch_down.start()
    wide_s[...] = other[...].astype(f32)
    compact(wide_s, rows_e, rows_d)
    fetch_gate.wait()
    gate_pre = gate_part[...] + mm(rows_e[...], gate[...])
    fetch_up.wait()
    up_pre = up_part[...] + mm(rows_e[...], up[...])
    hidden = clamped_unit(gate_pre, up_pre).astype(bf16)
    fetch_down.wait()
    total[...] = mm(hidden, down[...])
    out_mine[...] = total[:, pl.ds(at, half)].astype(bf16)
    out_other[...] = total[:, pl.ds(back, half)].astype(bf16)


def dense_kernel(core, mine, other, *refs):
    packs, out, gate_s, up_s, down_s = refs[:-4], refs[-4], refs[-3], refs[-2], refs[-1]
    half = mine.shape[1]
    units = packs[0].shape[0] // 3
    at = pl.multiple_of(core[0] * half, half)
    back = pl.multiple_of((1 - core[0]) * half, half)
    for i, pack in enumerate(packs):
        to = slice(i * units, (i + 1) * units)
        gate_s[to, :] = pack[0:units, :]
        up_s[to, :] = pack[units : 2 * units, :]
        down_s[to, :] = pack[2 * units : 3 * units, pl.ds(at, half)]
    rows, far = mine[...], other[...]
    gate = mm(rows, gate_s[:, pl.ds(at, half)], NT) + mm(far, gate_s[:, pl.ds(back, half)], NT)
    up = mm(rows, up_s[:, pl.ds(at, half)], NT) + mm(far, up_s[:, pl.ds(back, half)], NT)
    out[...] = mm(clamped_unit(gate, up).astype(bf16), down_s[...])


def join_kernel(dense, mine, other, out, wide_s):
    total = (mine[...].astype(f32) + other[...].astype(f32)).astype(bf16).astype(f32)
    spread(wide_s, total, 0)
    spread(wide_s, dense[...], CAP)
    out[...] = wide_s[...].astype(bf16)


def home_kernel(home_map, returned, kept, row_gate, out, wide_s, rows_s):
    seqs, half = kept.shape
    parts = half // LANES
    peers = rows_s.shape[0] // SLOTS
    wide_s[...] = returned[...].astype(f32)
    for r in range(SLOTS):
        for c in range(parts):
            rows_s[r * peers : (r + 1) * peers, c * LANES : (c + 1) * LANES] = gather(
                wide_s, r, c, parts, peers
            )
    sums = mm(home_map[...], rows_s[...])
    out[...] = (kept[...] + sums[:seqs] + row_gate[:, 0:1] * sums[seqs:]).astype(bf16)


def swap(array):
    return lax.ppermute(array, "tp", [(0, 1), (1, 0)])


def from_square(array):
    got = []
    for flip0, flip1 in ((1, 0), (0, 1), (1, 1)):
        pairs = [(4 * a + b, 4 * (a ^ flip0) + (b ^ flip1)) for a in range(4) for b in range(4)]
        got.append(lax.ppermute(array, ("ep_0", "ep_1"), pairs))
    return got


def shards(
    tokens, attn_gain, w_query1, w_query2, w_key1, w_key2, w_value, query_gain, key_gain,
    head_lambda, sub_gain, w_output, cache_key, cache_value, lengths, mix_gain, expert_gate,
    expert_up, expert_down, routes, route_weight, dense_mix, dense_gate, dense_up, dense_down,
):
    peers = lax.axis_size(EP)
    seqs, width = tokens.shape
    half, slots, wide = width // 2, CAP * peers, SLOTS * peers
    hidden = expert_gate.shape[2]
    core = lax.axis_index("tp").astype(jnp.int32).reshape(1)
    pack = jnp.concatenate([dense_gate.T, dense_up.T, dense_down], axis=0)
    packs = [pack] + from_square(pack)
    part, send_map, home_map = attention(
        tokens, attn_gain, w_query1, w_query2, w_key1, w_key2, w_value, query_gain,
        key_gain, head_lambda, sub_gain, w_output, cache_key, cache_value, lengths,
        routes, route_weight, peers,
    )
    block = (wide * half // LANES, LANES)
    send, kept, row_gate = call(
        mix_kernel,
        (
            core, tokens, part, swap(part), mix_gain.reshape(1, -1),
            dense_mix.reshape(-1, LANES), send_map,
        ),
        [(block, bf16), ((seqs, half), f32), ((seqs, LANES), f32)],
        [(block, f32)],
        2 * wide * seqs * half,
    )

    def exchange(blocks):
        blocks = blocks.reshape(peers, -1, LANES)
        return lax.all_to_all(blocks, EP, 0, 0, tiled=True).reshape(block)

    mine = exchange(send)
    other = swap(mine)
    rows_mine, gate_part, up_part = call(
        first_kernel,
        (core, mine, expert_gate, expert_up),
        [((DENSE_ROWS * peers, half), bf16)] + [((slots, hidden), f32)] * 2,
        [(block, f32), ((slots, half), bf16)] + [((half, hidden), bf16)] * 2,
        4 * slots * half * hidden,
        far=2,
    )
    rows_other, own, sent = call(
        second_kernel,
        (core, other, gate_part, up_part, expert_gate, expert_up, expert_down),
        [((DENSE_ROWS * peers, half), bf16)] + [((slots, half), bf16)] * 2,
        [(block, f32), ((slots, half), bf16), ((slots, width), f32)]
        + [((half, hidden), bf16)] * 2
        + [((hidden, width), bf16)],
        8 * slots * half * hidden,
        slots * hidden,
        far=3,
    )
    came = swap(sent)
    packs = packs + [swap(one) for one in packs]
    units = pack.shape[0] // 3 * len(packs)
    (dense,) = call(
        dense_kernel,
        (core, rows_mine, rows_other, *packs),
        [((DENSE_ROWS * peers, half), f32)],
        [((units, width), bf16), ((units, width), bf16), ((units, half), bf16)],
        10 * DENSE_ROWS * peers * half * units,
        DENSE_ROWS * peers * units,
    )
    (joined,) = call(join_kernel, (dense, own, came), [(block, bf16)], [(block, f32)], 0)
    returned = exchange(joined)
    (out,) = call(
        home_kernel,
        (home_map, returned, kept, row_gate),
        [((seqs, half), bf16)],
        [(block, f32), ((wide, half), bf16)],
        4 * seqs * wide * half,
    )
    return out


def solution(mesh):
    torus = Mesh(mesh.devices.reshape(4, 4, 4, mesh.shape["tp"]), EP_TP)
    in_specs = (
        P(EP, None), P(), P(None, "tp"), P(None, "tp"), P(None, "tp"), P(None, "tp"),
        P(None, "tp"), P(), P(), P("tp"), P(), P("tp", None), P(EP, "tp", None, None),
        P(EP, "tp", None, None), P(EP), P(), P(EP, None, "tp"), P(EP, None, "tp"),
        P(EP, "tp", None), P(EP, None), P(EP, None), P(), P(None, EP_TP), P(None, EP_TP),
        P(EP_TP, None),
    )
    return jax.shard_map(
        shards, mesh=torus, in_specs=in_specs, out_specs=P(EP, "tp"), check_vma=False
    )
```

```python
import functools

import jax
import jax.numpy as jnp
from jax import lax
from jax.experimental import pallas as pl
from jax.experimental.pallas import tpu as pltpu
from jax.sharding import Mesh
from jax.sharding import PartitionSpec as P


HEAD = 64
VHEAD = 128
EP = ("ep_0", "ep_1", "ep_2")
EP_TP = ("ep_0", "ep_1", "ep_2", "tp")
SLOTS = 6
CAP = 2
DENSE_ROWS = 4
LANES = 128
SEQ_STEP = 8
LIMIT = 40 << 20

epsilon = 1e-05
clamp_limit = 7.0
sigmoid_slope = 1.702
lambda_start = 0.2
neg_large = -1e30

bf16 = jnp.bfloat16
f32 = jnp.float32
NT = (((1,), (1,)), ((), ()))
TN = (((0,), (0,)), ((), ()))


def mm(a, b, dims=(((1,), (0,)), ((), ()))):
    return lax.dot_general(a, b, dims, preferred_element_type=f32)


def clamped_unit(gate_pre, up_pre):
    gate_pre = jnp.minimum(gate_pre, clamp_limit)
    up_pre = jnp.clip(up_pre, -clamp_limit, clamp_limit)
    return gate_pre * jax.nn.sigmoid(sigmoid_slope * gate_pre) * (up_pre + 1.0)


def rms(values):
    return lax.rsqrt(jnp.mean(values * values, axis=-1, keepdims=True) + epsilon)


def routing_maps(routes_t, weight_t, seqs, peers):
    wide = peers * SLOTS
    diag = lax.broadcasted_iota(jnp.int32, (seqs, seqs), 0) == lax.broadcasted_iota(
        jnp.int32, (seqs, seqs), 1
    )
    lane = lax.broadcasted_iota(jnp.int32, (seqs, wide), 1)
    peer, slot = lane % peers, lane // peers
    token = lax.broadcasted_iota(jnp.int32, (seqs, wide), 0)
    hit = jnp.zeros((seqs, wide), f32)
    weight = jnp.zeros((seqs, wide), f32)
    for k in range(routes_t.shape[0]):
        expert = jnp.sum(
            jnp.where(diag, routes_t[k : k + 1, :].astype(f32), 0.0), axis=1, keepdims=True
        ).astype(jnp.int32)
        share = jnp.sum(
            jnp.where(diag, weight_t[k : k + 1, :].astype(f32), 0.0), axis=1, keepdims=True
        )
        same = peer == expert
        hit = jnp.where(same, 1.0, hit)
        weight = jnp.where(same, share, weight)
    before = (
        lax.broadcasted_iota(jnp.int32, (seqs, seqs), 1)
        < lax.broadcasted_iota(jnp.int32, (seqs, seqs), 0)
    ).astype(bf16)
    rank = mm(before, hit.astype(bf16))
    chosen = (hit > 0.0) & (rank == slot.astype(f32)) & (slot < CAP)
    group = 2 * ((peer // 16) % 2) + (peer // 4) % 2
    dense = (token == group * DENSE_ROWS + slot - CAP) & (slot >= CAP)
    return (
        jnp.where(chosen | dense, 1.0, 0.0).astype(bf16),
        jnp.where(chosen, weight, 0.0).astype(bf16),
        jnp.where(dense, 1.0, 0.0).astype(bf16),
    )


def attention_kernel(*refs, peers):
    sources, refs = refs[:17], refs[17:]
    part, send_map, home_map = refs[:3]
    query_s, key_s, value_s, heads_s, *local = refs[3:-1]
    sems = refs[-1]
    (
        lengths, lam, tokens, attn_gain, w_query1, w_query2, w_key1, w_key2, w_value, query_gain, key_gain,
        routes_t, weight_t, sub_gain, w_output, cache_key, cache_value,
    ) = local
    seqs = tokens.shape[0]
    heads = w_query1.shape[1] // HEAD
    cached = cache_key.shape[2]
    rounds = seqs // SEQ_STEP
    copies = [
        pltpu.make_async_copy(sources[i], local[i], sems.at[i]) for i in range(len(local) - 2)
    ]
    chunks = []
    for b in range(rounds):
        of = pl.ds(b * SEQ_STEP, SEQ_STEP)
        for j in (0, 1):
            at = len(copies) + len(chunks)
            source, to = sources[15 + j].at[of], local[15 + j].at[of]
            chunks.append(pltpu.make_async_copy(source, to, sems.at[at]))
    for one in copies[:-1] + chunks + copies[-1:]:
        one.start()

    for one in copies[:-1]:
        one.wait()
    rows = tokens[...].astype(f32)
    normed = (rows * rms(rows) * attn_gain[...]).astype(bf16)
    nothing = jnp.zeros((seqs, HEAD), f32)
    for m, weight in enumerate((w_query1, w_query2)):
        query = mm(normed, weight[...])
        for h in range(heads):
            one = query[:, h * HEAD : (h + 1) * HEAD]
            one = (one * rms(one) * query_gain[...]).astype(bf16).astype(f32) * HEAD**-0.5
            pair = (one, nothing) if m == 0 else (nothing, one)
            at = (m * heads + h) * seqs
            query_s[at : at + seqs, :] = jnp.concatenate(pair, axis=1)
    new_keys = []
    for weight in (w_key1, w_key2):
        one = mm(normed, weight[...], NT)
        new_keys.append((one * rms(one) * key_gain[...]).astype(bf16).astype(f32))
    key_s[...] = jnp.concatenate(new_keys, axis=1)
    value_s[...] = mm(normed, w_value[...]).astype(bf16).astype(f32)
    send, routed, dense = routing_maps(routes_t[...], weight_t[...], seqs, peers)
    send_map[...] = send
    home_map[0:seqs, :] = routed
    home_map[seqs : 2 * seqs, :] = dense

    row = lax.broadcasted_iota(jnp.int32, (2 * heads, 1), 0)
    signed = jnp.ones((2 * heads, 1), f32)
    for h in range(heads):
        signed = jnp.where(row == heads + h, -lam[h], signed)
    lane = lax.broadcasted_iota(jnp.int32, (2 * heads, cached), 1)
    for b in range(rounds):
        span = range(b * SEQ_STEP, (b + 1) * SEQ_STEP)
        chunks[2 * b].wait()
        queries = [query_s[pl.ds(s, 2 * heads, stride=seqs), :] for s in span]
        fresh = [
            jnp.sum(query * key_s[s : s + 1, :], axis=1, keepdims=True)
            for s, query in zip(span, queries)
        ]
        scores = [
            jnp.where(lane < lengths[s], mm(query.astype(bf16), cache_key[s, 0], NT), neg_large)
            for s, query in zip(span, queries)
        ]
        top = [
            jnp.maximum(jnp.max(one, axis=1, keepdims=True), new)
            for one, new in zip(scores, fresh)
        ]
        expo = [jnp.exp(one - most) for one, most in zip(scores, top)]
        fresh_expo = [jnp.exp(one - most) for one, most in zip(fresh, top)]
        scale = [
            signed / (jnp.sum(one, axis=1, keepdims=True) + new)
            for one, new in zip(expo, fresh_expo)
        ]
        probs = [one * by for one, by in zip(expo, scale)]
        probs = [(one + pltpu.roll(one, heads, 0)).astype(bf16) for one in probs]
        chunks[2 * b + 1].wait()
        for s, one, new, by in zip(span, probs, fresh_expo, scale):
            new = new * by
            new = (new[0:heads] + new[heads:]).astype(bf16).astype(f32)
            heads_out = mm(one, cache_value[s, 0])[0:heads] + new * value_s[s : s + 1, :]
            heads_s[pl.ds(s, heads, stride=seqs), :] = heads_out

    subs = []
    for h in range(heads):
        one = heads_s[h * seqs : (h + 1) * seqs, :]
        subs.append((one * rms(one) * sub_gain[...] * (1.0 - lambda_start)).astype(bf16))
    copies[-1].wait()
    part[...] = mm(jnp.concatenate(subs, axis=1), w_output[...]).astype(bf16)


def attention(
    tokens, attn_gain, w_query1, w_query2, w_key1, w_key2, w_value, query_gain, key_gain,
    head_lambda, sub_gain, w_output, cache_key, cache_value, lengths, routes, route_weight,
    peers,
):
    seqs, width = tokens.shape
    heads = w_query1.shape[1] // HEAD
    cached = cache_key.shape[2]
    local = [
        lengths, head_lambda, tokens, attn_gain.reshape(1, -1), w_query1, w_query2, w_key1.T, w_key2.T, w_value,
        query_gain.reshape(1, -1), key_gain.reshape(1, -1), routes.T, route_weight.T,
        sub_gain.reshape(1, -1), w_output, cache_key, cache_value,
    ]
    flops = 2 * seqs * width * (2 * heads * HEAD + 2 * HEAD + VHEAD + heads * VHEAD)
    flops += 6 * seqs * 8 * cached * VHEAD
    wide = peers * SLOTS
    count = len(local) - 2 + 2 * (seqs // SEQ_STEP)
    return pl.pallas_call(
        functools.partial(attention_kernel, peers=peers),
        in_specs=[pl.BlockSpec(memory_space=pltpu.HBM)] * len(local),
        out_specs=[pl.BlockSpec(memory_space=pltpu.VMEM)] * 3,
        out_shape=[
            pltpu.VMEM((seqs, width), bf16),
            pltpu.VMEM((seqs, wide), bf16),
            pltpu.VMEM((2 * seqs, wide), bf16),
        ],
        scratch_shapes=[
            pltpu.VMEM((2 * heads * seqs, 2 * HEAD), f32),
            pltpu.VMEM((seqs, 2 * HEAD), f32),
            pltpu.VMEM((seqs, VHEAD), f32),
            pltpu.VMEM((heads * seqs, VHEAD), f32),
        ]
        + [pltpu.SMEM(one.shape, one.dtype) for one in local[:2]]
        + [pltpu.VMEM(one.shape, one.dtype) for one in local[2:]]
        + [pltpu.SemaphoreType.DMA((count,))],
        compiler_params=pltpu.CompilerParams(vmem_limit_bytes=LIMIT),
        cost_estimate=pl.CostEstimate(
            flops=flops, bytes_accessed=13 << 20, transcendentals=seqs * 8 * cached
        ),
        name="attention",
    )(*[pltpu.with_memory_space_constraint(one, pltpu.HBM) for one in local])


def spread(wide_s, rows, first):
    slots, peers, parts = wide_s.shape[0] // 64 // 8, 64, rows.shape[1] // LANES
    for r in range(rows.shape[0] // peers):
        for c in range(parts):
            wide_s[pl.ds((first + r) * parts + c, peers, stride=slots * parts), :] = rows[
                r * peers : (r + 1) * peers, c * LANES : (c + 1) * LANES
            ]


def gather(wide_s, r, c, parts, peers):
    slots = wide_s.shape[0] // peers // parts
    return wide_s[pl.ds(r * parts + c, peers, stride=slots * parts), :].astype(bf16)


def mix_kernel(core, tokens, mine, other, mix_gain, dense_mix, send_map, send, kept, row_gate, wide_s):
    half = kept.shape[1]
    attn_out = mine[...].astype(f32) + other[...].astype(f32)
    residual = (tokens[...].astype(f32) + attn_out).astype(bf16)
    rows = residual.astype(f32)
    mixed = (rows * rms(rows) * mix_gain[...]).astype(bf16).astype(f32)
    first = core[0] == 0
    kept[...] = jnp.where(first, rows[:, :half], rows[:, half:])
    gate = jnp.zeros((rows.shape[0], LANES), f32)
    for c in range(rows.shape[1] // LANES):
        gate = gate + mixed[:, c * LANES : (c + 1) * LANES] * dense_mix[c : c + 1, :].astype(f32)
    gate = jnp.sum(gate, axis=1, keepdims=True)
    row_gate[...] = jnp.broadcast_to(jax.nn.sigmoid(gate), row_gate.shape)
    columns = jnp.where(first, mixed[:, :half], mixed[:, half:]).astype(bf16)
    spread(wide_s, mm(send_map[...], columns, TN), 0)
    send[...] = wide_s[...].astype(bf16)


def call(kernel, args, outs, scratch, flops, transcendentals=0, far=0):
    near = len(args) - far
    spaces = [pltpu.SMEM if one.ndim == 1 else pltpu.VMEM for one in args[:near]]
    spaces += [pltpu.HBM] * far
    args = list(args[:near]) + [
        pltpu.with_memory_space_constraint(one, pltpu.HBM) for one in args[near:]
    ]
    out_shape = [jax.ShapeDtypeStruct(*one) for one in outs]
    moved = sum(one.size * one.dtype.itemsize for one in args + out_shape)
    return pl.pallas_call(
        kernel,
        in_specs=[pl.BlockSpec(memory_space=space) for space in spaces],
        out_specs=[pl.BlockSpec(memory_space=pltpu.VMEM)] * len(outs),
        out_shape=out_shape,
        scratch_shapes=[pltpu.VMEM(*one) for one in scratch]
        + [pltpu.SemaphoreType.DMA((far,))] * (far > 0),
        compiler_params=pltpu.CompilerParams(vmem_limit_bytes=LIMIT // 2),
        cost_estimate=pl.CostEstimate(
            flops=flops, bytes_accessed=moved, transcendentals=transcendentals
        ),
    )(*args)


def compact(wide_s, rows_e, rows_d):
    parts, peers = rows_d.shape[1] // LANES, rows_e.shape[0] // CAP
    for r in range(SLOTS):
        for c in range(parts):
            to, at = (rows_e, r) if r < CAP else (rows_d, r - CAP)
            to[at * peers : (at + 1) * peers, c * LANES : (c + 1) * LANES] = gather(
                wide_s, r, c, parts, peers
            )


def first_kernel(
    core, mine, gate_far, up_far, rows_d, gate_part, up_part, wide_s, rows_e, gate, up, sems
):
    half = rows_d.shape[1]
    own = pl.ds(pl.multiple_of(core[0] * half, half), half)
    fetch_gate = pltpu.make_async_copy(gate_far.at[0, own], gate, sems.at[0])
    fetch_up = pltpu.make_async_copy(up_far.at[0, own], up, sems.at[1])
    fetch_gate.start()
    fetch_up.start()
    wide_s[...] = mine[...].astype(f32)
    compact(wide_s, rows_e, rows_d)
    fetch_gate.wait()
    gate_part[...] = mm(rows_e[...], gate[...])
    fetch_up.wait()
    up_part[...] = mm(rows_e[...], up[...])


def second_kernel(
    core, other, gate_part, up_part, gate_far, up_far, down_far, rows_d, out_mine, out_other,
    wide_s, rows_e, total, gate, up, down, sems,
):
    half = rows_d.shape[1]
    at = pl.multiple_of(core[0] * half, half)
    back = pl.multiple_of((1 - core[0]) * half, half)
    fetch_gate = pltpu.make_async_copy(gate_far.at[0, pl.ds(back, half)], gate, sems.at[0])
    fetch_up = pltpu.make_async_copy(up_far.at[0, pl.ds(back, half)], up, sems.at[1])
    fetch_down = pltpu.make_async_copy(down_far.at[0], down, sems.at[2])
    fetch_gate.start()
    fetch_up.start()
    fetch_down.start()
    wide_s[...] = other[...].astype(f32)
    compact(wide_s, rows_e, rows_d)
    fetch_gate.wait()
    gate_pre = gate_part[...] + mm(rows_e[...], gate[...])
    fetch_up.wait()
    up_pre = up_part[...] + mm(rows_e[...], up[...])
    hidden = clamped_unit(gate_pre, up_pre).astype(bf16)
    fetch_down.wait()
    total[...] = mm(hidden, down[...])
    out_mine[...] = total[:, pl.ds(at, half)].astype(bf16)
    out_other[...] = total[:, pl.ds(back, half)].astype(bf16)


def dense_kernel(core, mine, other, *refs):
    packs, out, gate_s, up_s, down_s = refs[:-4], refs[-4], refs[-3], refs[-2], refs[-1]
    half = mine.shape[1]
    units = packs[0].shape[0] // 3
    at = pl.multiple_of(core[0] * half, half)
    back = pl.multiple_of((1 - core[0]) * half, half)
    for i, pack in enumerate(packs):
        to = slice(i * units, (i + 1) * units)
        gate_s[to, :] = pack[0:units, :]
        up_s[to, :] = pack[units : 2 * units, :]
        down_s[to, :] = pack[2 * units : 3 * units, pl.ds(at, half)]
    rows, far = mine[...], other[...]
    gate = mm(rows, gate_s[:, pl.ds(at, half)], NT) + mm(far, gate_s[:, pl.ds(back, half)], NT)
    up = mm(rows, up_s[:, pl.ds(at, half)], NT) + mm(far, up_s[:, pl.ds(back, half)], NT)
    out[...] = mm(clamped_unit(gate, up).astype(bf16), down_s[...])


def join_kernel(dense, mine, other, out, wide_s):
    total = (mine[...].astype(f32) + other[...].astype(f32)).astype(bf16).astype(f32)
    spread(wide_s, total, 0)
    spread(wide_s, dense[...], CAP)
    out[...] = wide_s[...].astype(bf16)


def home_kernel(home_map, returned, kept, row_gate, out, wide_s, rows_s):
    seqs, half = kept.shape
    parts = half // LANES
    peers = rows_s.shape[0] // SLOTS
    wide_s[...] = returned[...].astype(f32)
    for r in range(SLOTS):
        for c in range(parts):
            rows_s[r * peers : (r + 1) * peers, c * LANES : (c + 1) * LANES] = gather(
                wide_s, r, c, parts, peers
            )
    sums = mm(home_map[...], rows_s[...])
    out[...] = (kept[...] + sums[:seqs] + row_gate[:, 0:1] * sums[seqs:]).astype(bf16)


def swap(array):
    return lax.ppermute(array, "tp", [(0, 1), (1, 0)])


def from_square(array):
    got = []
    for flip0, flip1 in ((1, 0), (0, 1), (1, 1)):
        pairs = [(4 * a + b, 4 * (a ^ flip0) + (b ^ flip1)) for a in range(4) for b in range(4)]
        got.append(lax.ppermute(array, ("ep_0", "ep_1"), pairs))
    return got


def shards(
    tokens, attn_gain, w_query1, w_query2, w_key1, w_key2, w_value, query_gain, key_gain,
    head_lambda, sub_gain, w_output, cache_key, cache_value, lengths, mix_gain, expert_gate,
    expert_up, expert_down, routes, route_weight, dense_mix, dense_gate, dense_up, dense_down,
):
    peers = lax.axis_size(EP)
    seqs, width = tokens.shape
    half, slots, wide = width // 2, CAP * peers, SLOTS * peers
    hidden = expert_gate.shape[2]
    core = lax.axis_index("tp").astype(jnp.int32).reshape(1)
    pack = jnp.concatenate([dense_gate.T, dense_up.T, dense_down], axis=0)
    packs = [pack] + from_square(pack)
    part, send_map, home_map = attention(
        tokens, attn_gain, w_query1, w_query2, w_key1, w_key2, w_value, query_gain,
        key_gain, head_lambda, sub_gain, w_output, cache_key, cache_value, lengths,
        routes, route_weight, peers,
    )
    block = (wide * half // LANES, LANES)
    send, kept, row_gate = call(
        mix_kernel,
        (
            core, tokens, part, swap(part), mix_gain.reshape(1, -1),
            dense_mix.reshape(-1, LANES), send_map,
        ),
        [(block, bf16), ((seqs, half), f32), ((seqs, LANES), f32)],
        [(block, f32)],
        2 * wide * seqs * half,
    )

    def exchange(blocks):
        blocks = blocks.reshape(peers, -1, LANES)
        return lax.all_to_all(blocks, EP, 0, 0, tiled=True).reshape(block)

    mine = exchange(send)
    other = swap(mine)
    rows_mine, gate_part, up_part = call(
        first_kernel,
        (core, mine, expert_gate, expert_up),
        [((DENSE_ROWS * peers, half), bf16)] + [((slots, hidden), f32)] * 2,
        [(block, f32), ((slots, half), bf16)] + [((half, hidden), bf16)] * 2,
        4 * slots * half * hidden,
        far=2,
    )
    rows_other, own, sent = call(
        second_kernel,
        (core, other, gate_part, up_part, expert_gate, expert_up, expert_down),
        [((DENSE_ROWS * peers, half), bf16)] + [((slots, half), bf16)] * 2,
        [(block, f32), ((slots, half), bf16), ((slots, width), f32)]
        + [((half, hidden), bf16)] * 2
        + [((hidden, width), bf16)],
        8 * slots * half * hidden,
        slots * hidden,
        far=3,
    )
    came = swap(sent)
    packs = packs + [swap(one) for one in packs]
    units = pack.shape[0] // 3 * len(packs)
    (dense,) = call(
        dense_kernel,
        (core, rows_mine, rows_other, *packs),
        [((DENSE_ROWS * peers, half), f32)],
        [((units, width), bf16), ((units, width), bf16), ((units, half), bf16)],
        10 * DENSE_ROWS * peers * half * units,
        DENSE_ROWS * peers * units,
    )
    (joined,) = call(join_kernel, (dense, own, came), [(block, bf16)], [(block, f32)], 0)
    returned = exchange(joined)
    (out,) = call(
        home_kernel,
        (home_map, returned, kept, row_gate),
        [((seqs, half), bf16)],
        [(block, f32), ((wide, half), bf16)],
        4 * seqs * wide * half,
    )
    return out


def solution(mesh):
    torus = Mesh(mesh.devices.reshape(4, 4, 4, mesh.shape["tp"]), EP_TP)
    in_specs = (
        P(EP, None), P(), P(None, "tp"), P(None, "tp"), P(None, "tp"), P(None, "tp"),
        P(None, "tp"), P(), P(), P("tp"), P(), P("tp", None), P(EP, "tp", None, None),
        P(EP, "tp", None, None), P(EP), P(), P(EP, None, "tp"), P(EP, None, "tp"),
        P(EP, "tp", None), P(EP, None), P(EP, None), P(), P(None, EP_TP), P(None, EP_TP),
        P(EP_TP, None),
    )
    return jax.shard_map(
        shards, mesh=torus, in_specs=in_specs, out_specs=P(EP, "tp"), check_vma=False
    )
```

```python
import functools

import jax
import jax.numpy as jnp
from jax import lax
from jax.experimental import pallas as pl
from jax.experimental.pallas import tpu as pltpu
from jax.sharding import Mesh
from jax.sharding import PartitionSpec as P


HEAD = 64
VHEAD = 128
EP = ("ep_0", "ep_1", "ep_2")
EP_TP = ("ep_0", "ep_1", "ep_2", "tp")
SLOTS = 6
CAP = 2
DENSE_ROWS = 4
LANES = 128
SEQ_STEP = 8
LIMIT = 40 << 20

epsilon = 1e-05
clamp_limit = 7.0
sigmoid_slope = 1.702
lambda_start = 0.2
neg_large = -1e30

bf16 = jnp.bfloat16
f32 = jnp.float32
NT = (((1,), (1,)), ((), ()))
TN = (((0,), (0,)), ((), ()))


def mm(a, b, dims=(((1,), (0,)), ((), ()))):
    return lax.dot_general(a, b, dims, preferred_element_type=f32)


def clamped_unit(gate_pre, up_pre):
    gate_pre = jnp.minimum(gate_pre, clamp_limit)
    up_pre = jnp.clip(up_pre, -clamp_limit, clamp_limit)
    return gate_pre * jax.nn.sigmoid(sigmoid_slope * gate_pre) * (up_pre + 1.0)


def rms(values):
    return lax.rsqrt(jnp.mean(values * values, axis=-1, keepdims=True) + epsilon)


def routing_maps(routes_t, weight_t, seqs, peers):
    wide = peers * SLOTS
    diag = lax.broadcasted_iota(jnp.int32, (seqs, seqs), 0) == lax.broadcasted_iota(
        jnp.int32, (seqs, seqs), 1
    )
    lane = lax.broadcasted_iota(jnp.int32, (seqs, wide), 1)
    peer, slot = lane % peers, lane // peers
    token = lax.broadcasted_iota(jnp.int32, (seqs, wide), 0)
    hit = jnp.zeros((seqs, wide), f32)
    weight = jnp.zeros((seqs, wide), f32)
    for k in range(routes_t.shape[0]):
        expert = jnp.sum(
            jnp.where(diag, routes_t[k : k + 1, :].astype(f32), 0.0), axis=1, keepdims=True
        ).astype(jnp.int32)
        share = jnp.sum(
            jnp.where(diag, weight_t[k : k + 1, :].astype(f32), 0.0), axis=1, keepdims=True
        )
        same = peer == expert
        hit = jnp.where(same, 1.0, hit)
        weight = jnp.where(same, share, weight)
    before = (
        lax.broadcasted_iota(jnp.int32, (seqs, seqs), 1)
        < lax.broadcasted_iota(jnp.int32, (seqs, seqs), 0)
    ).astype(bf16)
    rank = mm(before, hit.astype(bf16))
    chosen = (hit > 0.0) & (rank == slot.astype(f32)) & (slot < CAP)
    group = 2 * ((peer // 16) % 2) + (peer // 4) % 2
    dense = (token == group * DENSE_ROWS + slot - CAP) & (slot >= CAP)
    return (
        jnp.where(chosen | dense, 1.0, 0.0).astype(bf16),
        jnp.where(chosen, weight, 0.0).astype(bf16),
        jnp.where(dense, 1.0, 0.0).astype(bf16),
    )


def attention_kernel(*refs, peers):
    sources, refs = refs[:17], refs[17:]
    part, send_map, home_map = refs[:3]
    query_s, key_s, value_s, heads_s, *local = refs[3:-1]
    sems = refs[-1]
    (
        lengths, lam, tokens, attn_gain, w_query1, w_query2, w_key1, w_key2, w_value, query_gain, key_gain,
        routes_t, weight_t, sub_gain, w_output, cache_key, cache_value,
    ) = local
    seqs = tokens.shape[0]
    heads = w_query1.shape[1] // HEAD
    cached = cache_key.shape[2]
    rounds = seqs // SEQ_STEP
    copies = [
        pltpu.make_async_copy(sources[i], local[i], sems.at[i]) for i in range(len(local) - 2)
    ]
    chunks = []
    for b in range(rounds):
        of = pl.ds(b * SEQ_STEP, SEQ_STEP)
        for j in (0, 1):
            at = len(copies) + len(chunks)
            source, to = sources[15 + j].at[of], local[15 + j].at[of]
            chunks.append(pltpu.make_async_copy(source, to, sems.at[at]))
    for one in copies[:-1] + chunks + copies[-1:]:
        one.start()

    for one in copies[:-1]:
        one.wait()
    rows = tokens[...].astype(f32)
    normed = (rows * rms(rows) * attn_gain[...]).astype(bf16)
    nothing = jnp.zeros((seqs, HEAD), f32)
    for m, weight in enumerate((w_query1, w_query2)):
        query = mm(normed, weight[...])
        for h in range(heads):
            one = query[:, h * HEAD : (h + 1) * HEAD]
            one = (one * rms(one) * query_gain[...]).astype(bf16).astype(f32) * HEAD**-0.5
            pair = (one, nothing) if m == 0 else (nothing, one)
            at = (m * heads + h) * seqs
            query_s[at : at + seqs, :] = jnp.concatenate(pair, axis=1)
    new_keys = []
    for weight in (w_key1, w_key2):
        one = mm(normed, weight[...], NT)
        new_keys.append((one * rms(one) * key_gain[...]).astype(bf16).astype(f32))
    key_s[...] = jnp.concatenate(new_keys, axis=1)
    value_s[...] = mm(normed, w_value[...]).astype(bf16).astype(f32)
    send, routed, dense = routing_maps(routes_t[...], weight_t[...], seqs, peers)
    send_map[...] = send
    home_map[0:seqs, :] = routed
    home_map[seqs : 2 * seqs, :] = dense

    row = lax.broadcasted_iota(jnp.int32, (2 * heads, 1), 0)
    signed = jnp.ones((2 * heads, 1), f32)
    for h in range(heads):
        signed = jnp.where(row == heads + h, -lam[h], signed)
    lane = lax.broadcasted_iota(jnp.int32, (2 * heads, cached), 1)
    for b in range(rounds):
        span = range(b * SEQ_STEP, (b + 1) * SEQ_STEP)
        chunks[2 * b].wait()
        queries = [query_s[pl.ds(s, 2 * heads, stride=seqs), :] for s in span]
        fresh = [
            jnp.sum(query * key_s[s : s + 1, :], axis=1, keepdims=True)
            for s, query in zip(span, queries)
        ]
        scores = [
            jnp.where(lane < lengths[s], mm(query.astype(bf16), cache_key[s, 0], NT), neg_large)
            for s, query in zip(span, queries)
        ]
        top = [
            jnp.maximum(jnp.max(one, axis=1, keepdims=True), new)
            for one, new in zip(scores, fresh)
        ]
        expo = [jnp.exp(one - most) for one, most in zip(scores, top)]
        fresh_expo = [jnp.exp(one - most) for one, most in zip(fresh, top)]
        scale = [
            signed / (jnp.sum(one, axis=1, keepdims=True) + new)
            for one, new in zip(expo, fresh_expo)
        ]
        probs = [one * by for one, by in zip(expo, scale)]
        probs = [(one + pltpu.roll(one, heads, 0)).astype(bf16) for one in probs]
        chunks[2 * b + 1].wait()
        for s, one, new, by in zip(span, probs, fresh_expo, scale):
            new = new * by
            new = (new[0:heads] + new[heads:]).astype(bf16).astype(f32)
            heads_out = mm(one, cache_value[s, 0])[0:heads] + new * value_s[s : s + 1, :]
            heads_s[pl.ds(s, heads, stride=seqs), :] = heads_out

    subs = []
    for h in range(heads):
        one = heads_s[h * seqs : (h + 1) * seqs, :]
        subs.append((one * rms(one) * sub_gain[...] * (1.0 - lambda_start)).astype(bf16))
    copies[-1].wait()
    part[...] = mm(jnp.concatenate(subs, axis=1), w_output[...]).astype(bf16)


def attention(
    tokens, attn_gain, w_query1, w_query2, w_key1, w_key2, w_value, query_gain, key_gain,
    head_lambda, sub_gain, w_output, cache_key, cache_value, lengths, routes, route_weight,
    peers,
):
    seqs, width = tokens.shape
    heads = w_query1.shape[1] // HEAD
    cached = cache_key.shape[2]
    local = [
        lengths, head_lambda, tokens, attn_gain.reshape(1, -1), w_query1, w_query2, w_key1.T, w_key2.T, w_value,
        query_gain.reshape(1, -1), key_gain.reshape(1, -1), routes.T, route_weight.T,
        sub_gain.reshape(1, -1), w_output, cache_key, cache_value,
    ]
    flops = 2 * seqs * width * (2 * heads * HEAD + 2 * HEAD + VHEAD + heads * VHEAD)
    flops += 6 * seqs * 8 * cached * VHEAD
    wide = peers * SLOTS
    count = len(local) - 2 + 2 * (seqs // SEQ_STEP)
    return pl.pallas_call(
        functools.partial(attention_kernel, peers=peers),
        in_specs=[pl.BlockSpec(memory_space=pltpu.HBM)] * len(local),
        out_specs=[pl.BlockSpec(memory_space=pltpu.VMEM)] * 3,
        out_shape=[
            pltpu.VMEM((seqs, width), bf16),
            pltpu.VMEM((seqs, wide), bf16),
            pltpu.VMEM((2 * seqs, wide), bf16),
        ],
        scratch_shapes=[
            pltpu.VMEM((2 * heads * seqs, 2 * HEAD), f32),
            pltpu.VMEM((seqs, 2 * HEAD), f32),
            pltpu.VMEM((seqs, VHEAD), f32),
            pltpu.VMEM((heads * seqs, VHEAD), f32),
        ]
        + [pltpu.SMEM(one.shape, one.dtype) for one in local[:2]]
        + [pltpu.VMEM(one.shape, one.dtype) for one in local[2:]]
        + [pltpu.SemaphoreType.DMA((count,))],
        compiler_params=pltpu.CompilerParams(vmem_limit_bytes=LIMIT),
        cost_estimate=pl.CostEstimate(
            flops=flops, bytes_accessed=13 << 20, transcendentals=seqs * 8 * cached
        ),
        name="attention",
    )(*[pltpu.with_memory_space_constraint(one, pltpu.HBM) for one in local])


def spread(wide_s, rows, first):
    slots, peers, parts = wide_s.shape[0] // 64 // 8, 64, rows.shape[1] // LANES
    for r in range(rows.shape[0] // peers):
        for c in range(parts):
            wide_s[pl.ds((first + r) * parts + c, peers, stride=slots * parts), :] = rows[
                r * peers : (r + 1) * peers, c * LANES : (c + 1) * LANES
            ]


def gather(wide_s, r, c, parts, peers):
    slots = wide_s.shape[0] // peers // parts
    return wide_s[pl.ds(r * parts + c, peers, stride=slots * parts), :].astype(bf16)


def mix_kernel(core, tokens, mine, other, mix_gain, dense_mix, send_map, send, kept, row_gate, wide_s):
    half = kept.shape[1]
    attn_out = mine[...].astype(f32) + other[...].astype(f32)
    residual = (tokens[...].astype(f32) + attn_out).astype(bf16)
    rows = residual.astype(f32)
    mixed = (rows * rms(rows) * mix_gain[...]).astype(bf16).astype(f32)
    first = core[0] == 0
    kept[...] = jnp.where(first, rows[:, :half], rows[:, half:])
    gate = jnp.zeros((rows.shape[0], LANES), f32)
    for c in range(rows.shape[1] // LANES):
        gate = gate + mixed[:, c * LANES : (c + 1) * LANES] * dense_mix[c : c + 1, :].astype(f32)
    gate = jnp.sum(gate, axis=1, keepdims=True)
    row_gate[...] = jnp.broadcast_to(jax.nn.sigmoid(gate), row_gate.shape)
    columns = jnp.where(first, mixed[:, :half], mixed[:, half:]).astype(bf16)
    spread(wide_s, mm(send_map[...], columns, TN), 0)
    send[...] = wide_s[...].astype(bf16)


def call(kernel, args, outs, scratch, flops, transcendentals=0, far=0):
    near = len(args) - far
    spaces = [pltpu.SMEM if one.ndim == 1 else pltpu.VMEM for one in args[:near]]
    spaces += [pltpu.HBM] * far
    args = list(args[:near]) + [
        pltpu.with_memory_space_constraint(one, pltpu.HBM) for one in args[near:]
    ]
    out_shape = [jax.ShapeDtypeStruct(*one) for one in outs]
    moved = sum(one.size * one.dtype.itemsize for one in args + out_shape)
    return pl.pallas_call(
        kernel,
        in_specs=[pl.BlockSpec(memory_space=space) for space in spaces],
        out_specs=[pl.BlockSpec(memory_space=pltpu.VMEM)] * len(outs),
        out_shape=out_shape,
        scratch_shapes=[pltpu.VMEM(*one) for one in scratch]
        + [pltpu.SemaphoreType.DMA((far,))] * (far > 0),
        compiler_params=pltpu.CompilerParams(vmem_limit_bytes=LIMIT // 2),
        cost_estimate=pl.CostEstimate(
            flops=flops, bytes_accessed=moved, transcendentals=transcendentals
        ),
    )(*args)


def compact(wide_s, rows_e, rows_d):
    parts, peers = rows_d.shape[1] // LANES, rows_e.shape[0] // CAP
    for r in range(SLOTS):
        for c in range(parts):
            to, at = (rows_e, r) if r < CAP else (rows_d, r - CAP)
            to[at * peers : (at + 1) * peers, c * LANES : (c + 1) * LANES] = gather(
                wide_s, r, c, parts, peers
            )


def first_kernel(
    core, mine, gate_far, up_far, rows_d, gate_part, up_part, wide_s, rows_e, gate, up, sems
):
    half = rows_d.shape[1]
    own = pl.ds(pl.multiple_of(core[0] * half, half), half)
    fetch_gate = pltpu.make_async_copy(gate_far.at[0, own], gate, sems.at[0])
    fetch_up = pltpu.make_async_copy(up_far.at[0, own], up, sems.at[1])
    fetch_gate.start()
    fetch_up.start()
    wide_s[...] = mine[...].astype(f32)
    compact(wide_s, rows_e, rows_d)
    fetch_gate.wait()
    gate_part[...] = mm(rows_e[...], gate[...])
    fetch_up.wait()
    up_part[...] = mm(rows_e[...], up[...])


def second_kernel(
    core, other, gate_part, up_part, gate_far, up_far, down_far, rows_d, out_mine, out_other,
    wide_s, rows_e, total, gate, up, down, sems,
):
    half = rows_d.shape[1]
    at = pl.multiple_of(core[0] * half, half)
    back = pl.multiple_of((1 - core[0]) * half, half)
    fetch_gate = pltpu.make_async_copy(gate_far.at[0, pl.ds(back, half)], gate, sems.at[0])
    fetch_up = pltpu.make_async_copy(up_far.at[0, pl.ds(back, half)], up, sems.at[1])
    fetch_down = pltpu.make_async_copy(down_far.at[0], down, sems.at[2])
    fetch_gate.start()
    fetch_up.start()
    fetch_down.start()
    wide_s[...] = other[...].astype(f32)
    compact(wide_s, rows_e, rows_d)
    fetch_gate.wait()
    gate_pre = gate_part[...] + mm(rows_e[...], gate[...])
    fetch_up.wait()
    up_pre = up_part[...] + mm(rows_e[...], up[...])
    hidden = clamped_unit(gate_pre, up_pre).astype(bf16)
    fetch_down.wait()
    total[...] = mm(hidden, down[...])
    out_mine[...] = total[:, pl.ds(at, half)].astype(bf16)
    out_other[...] = total[:, pl.ds(back, half)].astype(bf16)


def dense_kernel(core, mine, other, *refs):
    packs, out, gate_s, up_s, down_s = refs[:-4], refs[-4], refs[-3], refs[-2], refs[-1]
    half = mine.shape[1]
    units = packs[0].shape[0] // 3
    at = pl.multiple_of(core[0] * half, half)
    back = pl.multiple_of((1 - core[0]) * half, half)
    for i, pack in enumerate(packs):
        to = slice(i * units, (i + 1) * units)
        gate_s[to, :] = pack[0:units, :]
        up_s[to, :] = pack[units : 2 * units, :]
        down_s[to, :] = pack[2 * units : 3 * units, pl.ds(at, half)]
    rows, far = mine[...], other[...]
    gate = mm(rows, gate_s[:, pl.ds(at, half)], NT) + mm(far, gate_s[:, pl.ds(back, half)], NT)
    up = mm(rows, up_s[:, pl.ds(at, half)], NT) + mm(far, up_s[:, pl.ds(back, half)], NT)
    out[...] = mm(clamped_unit(gate, up).astype(bf16), down_s[...])


def join_kernel(dense, mine, other, out, wide_s):
    total = (mine[...].astype(f32) + other[...].astype(f32)).astype(bf16).astype(f32)
    spread(wide_s, total, 0)
    spread(wide_s, dense[...], CAP)
    out[...] = wide_s[...].astype(bf16)


def home_kernel(home_map, returned, kept, row_gate, out, wide_s, rows_s):
    seqs, half = kept.shape
    parts = half // LANES
    peers = rows_s.shape[0] // SLOTS
    wide_s[...] = returned[...].astype(f32)
    for r in range(SLOTS):
        for c in range(parts):
            rows_s[r * peers : (r + 1) * peers, c * LANES : (c + 1) * LANES] = gather(
                wide_s, r, c, parts, peers
            )
    sums = mm(home_map[...], rows_s[...])
    out[...] = (kept[...] + sums[:seqs] + row_gate[:, 0:1] * sums[seqs:]).astype(bf16)


def swap(array):
    return lax.ppermute(array, "tp", [(0, 1), (1, 0)])


def across(array, turn):
    pairs = []
    for a in range(4):
        for b in range(4):
            for t in range(2):
                flip = (t + turn) % 2
                to = 4 * (a ^ (1 - flip)) + (b ^ flip)
                pairs.append((2 * (4 * a + b) + t, 2 * to + t))
    return lax.ppermute(array, ("ep_0", "ep_1", "tp"), pairs)


def shards(
    tokens, attn_gain, w_query1, w_query2, w_key1, w_key2, w_value, query_gain, key_gain,
    head_lambda, sub_gain, w_output, cache_key, cache_value, lengths, mix_gain, expert_gate,
    expert_up, expert_down, routes, route_weight, dense_mix, dense_gate, dense_up, dense_down,
):
    peers = lax.axis_size(EP)
    seqs, width = tokens.shape
    half, slots, wide = width // 2, CAP * peers, SLOTS * peers
    hidden = expert_gate.shape[2]
    core = lax.axis_index("tp").astype(jnp.int32).reshape(1)
    pack = jnp.concatenate([dense_gate.T, dense_up.T, dense_down], axis=0)
    pack0 = across(pack, 0)
    part, send_map, home_map = attention(
        tokens, attn_gain, w_query1, w_query2, w_key1, w_key2, w_value, query_gain,
        key_gain, head_lambda, sub_gain, w_output, cache_key, cache_value, lengths,
        routes, route_weight, peers,
    )
    block = (wide * half // LANES, LANES)
    far = swap(part)
    pack1 = across(pack, 1)
    pack2 = across(pack0, 1)
    send, kept, row_gate = call(
        mix_kernel,
        (
            core, tokens, part, far, mix_gain.reshape(1, -1),
            dense_mix.reshape(-1, LANES), send_map,
        ),
        [(block, bf16), ((seqs, half), f32), ((seqs, LANES), f32)],
        [(block, f32)],
        2 * wide * seqs * half,
    )

    def exchange(blocks):
        blocks = blocks.reshape(peers, -1, LANES)
        return lax.all_to_all(blocks, EP, 0, 0, tiled=True).reshape(block)

    mine = exchange(send)
    other = swap(mine)
    rows_mine, gate_part, up_part = call(
        first_kernel,
        (core, mine, expert_gate, expert_up),
        [((DENSE_ROWS * peers, half), bf16)] + [((slots, hidden), f32)] * 2,
        [(block, f32), ((slots, half), bf16)] + [((half, hidden), bf16)] * 2,
        4 * slots * half * hidden,
        far=2,
    )
    rows_other, own, sent = call(
        second_kernel,
        (core, other, gate_part, up_part, expert_gate, expert_up, expert_down),
        [((DENSE_ROWS * peers, half), bf16)] + [((slots, half), bf16)] * 2,
        [(block, f32), ((slots, half), bf16), ((slots, width), f32)]
        + [((half, hidden), bf16)] * 2
        + [((hidden, width), bf16)],
        8 * slots * half * hidden,
        slots * hidden,
        far=3,
    )
    came = swap(sent)
    packs = [pack, pack0, pack1, pack2]
    packs = packs + [swap(one) for one in packs]
    units = pack.shape[0] // 3 * len(packs)
    (dense,) = call(
        dense_kernel,
        (core, rows_mine, rows_other, *packs),
        [((DENSE_ROWS * peers, half), f32)],
        [((units, width), bf16), ((units, width), bf16), ((units, half), bf16)],
        10 * DENSE_ROWS * peers * half * units,
        DENSE_ROWS * peers * units,
    )
    (joined,) = call(join_kernel, (dense, own, came), [(block, bf16)], [(block, f32)], 0)
    returned = exchange(joined)
    (out,) = call(
        home_kernel,
        (home_map, returned, kept, row_gate),
        [((seqs, half), bf16)],
        [(block, f32), ((wide, half), bf16)],
        4 * seqs * wide * half,
    )
    return out


def solution(mesh):
    torus = Mesh(mesh.devices.reshape(4, 4, 4, mesh.shape["tp"]), EP_TP)
    in_specs = (
        P(EP, None), P(), P(None, "tp"), P(None, "tp"), P(None, "tp"), P(None, "tp"),
        P(None, "tp"), P(), P(), P("tp"), P(), P("tp", None), P(EP, "tp", None, None),
        P(EP, "tp", None, None), P(EP), P(), P(EP, None, "tp"), P(EP, None, "tp"),
        P(EP, "tp", None), P(EP, None), P(EP, None), P(), P(None, EP_TP), P(None, EP_TP),
        P(EP_TP, None),
    )
    return jax.shard_map(
        shards, mesh=torus, in_specs=in_specs, out_specs=P(EP, "tp"), check_vma=False
    )
```

```python
import functools

import jax
import jax.numpy as jnp
from jax import lax
from jax.experimental import pallas as pl
from jax.experimental.pallas import tpu as pltpu
from jax.sharding import Mesh
from jax.sharding import PartitionSpec as P


HEAD = 64
VHEAD = 128
EP = ("ep_0", "ep_1", "ep_2")
EP_TP = ("ep_0", "ep_1", "ep_2", "tp")
SLOTS = 6
CAP = 2
DENSE_ROWS = 4
LANES = 128
SEQ_STEP = 8
LIMIT = 40 << 20

epsilon = 1e-05
clamp_limit = 7.0
sigmoid_slope = 1.702
lambda_start = 0.2
neg_large = -1e30

bf16 = jnp.bfloat16
f32 = jnp.float32
NT = (((1,), (1,)), ((), ()))
TN = (((0,), (0,)), ((), ()))


def mm(a, b, dims=(((1,), (0,)), ((), ()))):
    return lax.dot_general(a, b, dims, preferred_element_type=f32)


def clamped_unit(gate_pre, up_pre):
    gate_pre = jnp.minimum(gate_pre, clamp_limit)
    up_pre = jnp.clip(up_pre, -clamp_limit, clamp_limit)
    return gate_pre * jax.nn.sigmoid(sigmoid_slope * gate_pre) * (up_pre + 1.0)


def rms(values):
    return lax.rsqrt(jnp.mean(values * values, axis=-1, keepdims=True) + epsilon)


def routing_maps(routes_t, weight_t, seqs, peers):
    wide = peers * SLOTS
    diag = lax.broadcasted_iota(jnp.int32, (seqs, seqs), 0) == lax.broadcasted_iota(
        jnp.int32, (seqs, seqs), 1
    )
    lane = lax.broadcasted_iota(jnp.int32, (seqs, wide), 1)
    peer, slot = lane % peers, lane // peers
    token = lax.broadcasted_iota(jnp.int32, (seqs, wide), 0)
    hit = jnp.zeros((seqs, wide), f32)
    weight = jnp.zeros((seqs, wide), f32)
    for k in range(routes_t.shape[0]):
        expert = jnp.sum(
            jnp.where(diag, routes_t[k : k + 1, :].astype(f32), 0.0), axis=1, keepdims=True
        ).astype(jnp.int32)
        share = jnp.sum(
            jnp.where(diag, weight_t[k : k + 1, :].astype(f32), 0.0), axis=1, keepdims=True
        )
        same = peer == expert
        hit = jnp.where(same, 1.0, hit)
        weight = jnp.where(same, share, weight)
    before = (
        lax.broadcasted_iota(jnp.int32, (seqs, seqs), 1)
        < lax.broadcasted_iota(jnp.int32, (seqs, seqs), 0)
    ).astype(bf16)
    rank = mm(before, hit.astype(bf16))
    chosen = (hit > 0.0) & (rank == slot.astype(f32)) & (slot < CAP)
    group = 2 * ((peer // 16) % 2) + (peer // 4) % 2
    dense = (token == group * DENSE_ROWS + slot - CAP) & (slot >= CAP)
    return (
        jnp.where(chosen | dense, 1.0, 0.0).astype(bf16),
        jnp.where(chosen, weight, 0.0).astype(bf16),
        jnp.where(dense, 1.0, 0.0).astype(bf16),
    )


def attention_kernel(*refs, peers):
    sources, refs = refs[:17], refs[17:]
    part, send_map, home_map = refs[:3]
    query_s, key_s, value_s, heads_s, *local = refs[3:-1]
    sems = refs[-1]
    (
        lengths, lam, tokens, attn_gain, w_query1, w_query2, w_key1, w_key2, w_value, query_gain, key_gain,
        routes_t, weight_t, sub_gain, w_output, cache_key, cache_value,
    ) = local
    seqs = tokens.shape[0]
    heads = w_query1.shape[1] // HEAD
    cached = cache_key.shape[2]
    rounds = seqs // SEQ_STEP
    copies = [
        pltpu.make_async_copy(sources[i], local[i], sems.at[i]) for i in range(len(local) - 2)
    ]
    chunks = []
    for b in range(rounds):
        of = pl.ds(b * SEQ_STEP, SEQ_STEP)
        for j in (0, 1):
            at = len(copies) + len(chunks)
            source, to = sources[15 + j].at[of], local[15 + j].at[of]
            chunks.append(pltpu.make_async_copy(source, to, sems.at[at]))
    for one in copies[:-1] + chunks + copies[-1:]:
        one.start()

    for one in copies[:-1]:
        one.wait()
    rows = tokens[...].astype(f32)
    normed = (rows * rms(rows) * attn_gain[...]).astype(bf16)
    nothing = jnp.zeros((seqs, HEAD), f32)
    for m, weight in enumerate((w_query1, w_query2)):
        query = mm(normed, weight[...])
        for h in range(heads):
            one = query[:, h * HEAD : (h + 1) * HEAD]
            one = (one * rms(one) * query_gain[...]).astype(bf16).astype(f32) * HEAD**-0.5
            pair = (one, nothing) if m == 0 else (nothing, one)
            at = (m * heads + h) * seqs
            query_s[at : at + seqs, :] = jnp.concatenate(pair, axis=1)
    new_keys = []
    for weight in (w_key1, w_key2):
        one = mm(normed, weight[...], NT)
        new_keys.append((one * rms(one) * key_gain[...]).astype(bf16).astype(f32))
    key_s[...] = jnp.concatenate(new_keys, axis=1)
    value_s[...] = mm(normed, w_value[...]).astype(bf16).astype(f32)
    send, routed, dense = routing_maps(routes_t[...], weight_t[...], seqs, peers)
    send_map[...] = send
    home_map[0:seqs, :] = routed
    home_map[seqs : 2 * seqs, :] = dense

    row = lax.broadcasted_iota(jnp.int32, (2 * heads, 1), 0)
    signed = jnp.ones((2 * heads, 1), f32)
    for h in range(heads):
        signed = jnp.where(row == heads + h, -lam[h], signed)
    lane = lax.broadcasted_iota(jnp.int32, (2 * heads, cached), 1)
    for b in range(rounds):
        span = range(b * SEQ_STEP, (b + 1) * SEQ_STEP)
        chunks[2 * b].wait()
        queries = [query_s[pl.ds(s, 2 * heads, stride=seqs), :] for s in span]
        fresh = [
            jnp.sum(query * key_s[s : s + 1, :], axis=1, keepdims=True)
            for s, query in zip(span, queries)
        ]
        scores = [
            jnp.where(lane < lengths[s], mm(query.astype(bf16), cache_key[s, 0], NT), neg_large)
            for s, query in zip(span, queries)
        ]
        top = [
            jnp.maximum(jnp.max(one, axis=1, keepdims=True), new)
            for one, new in zip(scores, fresh)
        ]
        expo = [jnp.exp(one - most) for one, most in zip(scores, top)]
        fresh_expo = [jnp.exp(one - most) for one, most in zip(fresh, top)]
        scale = [
            signed / (jnp.sum(one, axis=1, keepdims=True) + new)
            for one, new in zip(expo, fresh_expo)
        ]
        probs = [one * by for one, by in zip(expo, scale)]
        probs = [(one + pltpu.roll(one, heads, 0)).astype(bf16) for one in probs]
        chunks[2 * b + 1].wait()
        for s, one, new, by in zip(span, probs, fresh_expo, scale):
            new = new * by
            new = (new[0:heads] + new[heads:]).astype(bf16).astype(f32)
            heads_out = mm(one, cache_value[s, 0])[0:heads] + new * value_s[s : s + 1, :]
            heads_s[pl.ds(s, heads, stride=seqs), :] = heads_out

    subs = []
    for h in range(heads):
        one = heads_s[h * seqs : (h + 1) * seqs, :]
        subs.append((one * rms(one) * sub_gain[...] * (1.0 - lambda_start)).astype(bf16))
    copies[-1].wait()
    part[...] = mm(jnp.concatenate(subs, axis=1), w_output[...]).astype(bf16)


def attention(
    tokens, attn_gain, w_query1, w_query2, w_key1, w_key2, w_value, query_gain, key_gain,
    head_lambda, sub_gain, w_output, cache_key, cache_value, lengths, routes, route_weight,
    peers,
):
    seqs, width = tokens.shape
    heads = w_query1.shape[1] // HEAD
    cached = cache_key.shape[2]
    local = [
        lengths, head_lambda, tokens, attn_gain.reshape(1, -1), w_query1, w_query2, w_key1.T, w_key2.T, w_value,
        query_gain.reshape(1, -1), key_gain.reshape(1, -1), routes.T, route_weight.T,
        sub_gain.reshape(1, -1), w_output, cache_key, cache_value,
    ]
    flops = 2 * seqs * width * (2 * heads * HEAD + 2 * HEAD + VHEAD + heads * VHEAD)
    flops += 6 * seqs * 8 * cached * VHEAD
    wide = peers * SLOTS
    count = len(local) - 2 + 2 * (seqs // SEQ_STEP)
    return pl.pallas_call(
        functools.partial(attention_kernel, peers=peers),
        in_specs=[pl.BlockSpec(memory_space=pltpu.HBM)] * len(local),
        out_specs=[pl.BlockSpec(memory_space=pltpu.VMEM)] * 3,
        out_shape=[
            pltpu.VMEM((seqs, width), bf16),
            pltpu.VMEM((seqs, wide), bf16),
            pltpu.VMEM((2 * seqs, wide), bf16),
        ],
        scratch_shapes=[
            pltpu.VMEM((2 * heads * seqs, 2 * HEAD), f32),
            pltpu.VMEM((seqs, 2 * HEAD), f32),
            pltpu.VMEM((seqs, VHEAD), f32),
            pltpu.VMEM((heads * seqs, VHEAD), f32),
        ]
        + [pltpu.SMEM(one.shape, one.dtype) for one in local[:2]]
        + [pltpu.VMEM(one.shape, one.dtype) for one in local[2:]]
        + [pltpu.SemaphoreType.DMA((count,))],
        compiler_params=pltpu.CompilerParams(vmem_limit_bytes=LIMIT),
        cost_estimate=pl.CostEstimate(
            flops=flops, bytes_accessed=13 << 20, transcendentals=seqs * 8 * cached
        ),
        name="attention",
    )(*[pltpu.with_memory_space_constraint(one, pltpu.HBM) for one in local])


def spread(wide_s, rows, first):
    slots, peers, parts = wide_s.shape[0] // 64 // 8, 64, rows.shape[1] // LANES
    for r in range(rows.shape[0] // peers):
        for c in range(parts):
            wide_s[pl.ds((first + r) * parts + c, peers, stride=slots * parts), :] = rows[
                r * peers : (r + 1) * peers, c * LANES : (c + 1) * LANES
            ]


def gather(wide_s, r, c, parts, peers):
    slots = wide_s.shape[0] // peers // parts
    return wide_s[pl.ds(r * parts + c, peers, stride=slots * parts), :].astype(bf16)


def mix_kernel(core, tokens, mine, other, mix_gain, dense_mix, send_map, send, kept, row_gate, wide_s):
    half = kept.shape[1]
    attn_out = mine[...].astype(f32) + other[...].astype(f32)
    residual = (tokens[...].astype(f32) + attn_out).astype(bf16)
    rows = residual.astype(f32)
    mixed = (rows * rms(rows) * mix_gain[...]).astype(bf16).astype(f32)
    first = core[0] == 0
    kept[...] = jnp.where(first, rows[:, :half], rows[:, half:])
    gate = jnp.zeros((rows.shape[0], LANES), f32)
    for c in range(rows.shape[1] // LANES):
        gate = gate + mixed[:, c * LANES : (c + 1) * LANES] * dense_mix[c : c + 1, :].astype(f32)
    gate = jnp.sum(gate, axis=1, keepdims=True)
    row_gate[...] = jnp.broadcast_to(jax.nn.sigmoid(gate), row_gate.shape)
    columns = jnp.where(first, mixed[:, :half], mixed[:, half:]).astype(bf16)
    spread(wide_s, mm(send_map[...], columns, TN), 0)
    send[...] = wide_s[...].astype(bf16)


def call(kernel, args, outs, scratch, flops, transcendentals=0, far=0, sems=0):
    near = len(args) - far
    spaces = [pltpu.SMEM if one.ndim == 1 else pltpu.VMEM for one in args[:near]]
    spaces += [pltpu.HBM] * far
    args = list(args[:near]) + [
        pltpu.with_memory_space_constraint(one, pltpu.HBM) for one in args[near:]
    ]
    out_shape = [jax.ShapeDtypeStruct(*one) for one in outs]
    moved = sum(one.size * one.dtype.itemsize for one in args + out_shape)
    return pl.pallas_call(
        kernel,
        in_specs=[pl.BlockSpec(memory_space=space) for space in spaces],
        out_specs=[pl.BlockSpec(memory_space=pltpu.VMEM)] * len(outs),
        out_shape=out_shape,
        scratch_shapes=[pltpu.VMEM(*one) for one in scratch]
        + [pltpu.SemaphoreType.DMA((sems,))] * (sems > 0),
        compiler_params=pltpu.CompilerParams(vmem_limit_bytes=LIMIT // 2),
        cost_estimate=pl.CostEstimate(
            flops=flops, bytes_accessed=moved, transcendentals=transcendentals
        ),
    )(*args)


def compact(wide_s, rows_e, rows_d):
    parts, peers = rows_d.shape[1] // LANES, rows_e.shape[0] // CAP
    for r in range(SLOTS):
        for c in range(parts):
            to, at = (rows_e, r) if r < CAP else (rows_d, r - CAP)
            to[at * peers : (at + 1) * peers, c * LANES : (c + 1) * LANES] = gather(
                wide_s, r, c, parts, peers
            )


def first_kernel(
    core, mine, gate_far, up_far, rows_d, gate_part, up_part, gate_back, up_back,
    wide_s, rows_e, gate, up, sems,
):
    half = rows_d.shape[1]
    own = pl.ds(pl.multiple_of(core[0] * half, half), half)
    back = pl.ds(pl.multiple_of((1 - core[0]) * half, half), half)
    fetch_gate = pltpu.make_async_copy(gate_far.at[0, own], gate, sems.at[0])
    fetch_up = pltpu.make_async_copy(up_far.at[0, own], up, sems.at[1])
    later = [
        pltpu.make_async_copy(gate_far.at[0, back], gate_back, sems.at[2]),
        pltpu.make_async_copy(up_far.at[0, back], up_back, sems.at[3]),
    ]
    for one in [fetch_gate, fetch_up] + later:
        one.start()
    wide_s[...] = mine[...].astype(f32)
    compact(wide_s, rows_e, rows_d)
    fetch_gate.wait()
    gate_part[...] = mm(rows_e[...], gate[...])
    fetch_up.wait()
    up_part[...] = mm(rows_e[...], up[...])
    for one in later:
        one.wait()


def second_kernel(
    core, other, gate_part, up_part, gate, up, down, rows_d, out_mine, out_other,
    wide_s, rows_e, total,
):
    half = rows_d.shape[1]
    at = pl.multiple_of(core[0] * half, half)
    back = pl.multiple_of((1 - core[0]) * half, half)
    wide_s[...] = other[...].astype(f32)
    compact(wide_s, rows_e, rows_d)
    gate_pre = gate_part[...] + mm(rows_e[...], gate[...])
    up_pre = up_part[...] + mm(rows_e[...], up[...])
    hidden = clamped_unit(gate_pre, up_pre).astype(bf16)
    total[...] = mm(hidden, down[0])
    out_mine[...] = total[:, pl.ds(at, half)].astype(bf16)
    out_other[...] = total[:, pl.ds(back, half)].astype(bf16)


def dense_kernel(core, mine, other, *refs):
    packs, out, gate_s, up_s, down_s = refs[:-4], refs[-4], refs[-3], refs[-2], refs[-1]
    half = mine.shape[1]
    units = packs[0].shape[0] // 3
    at = pl.multiple_of(core[0] * half, half)
    back = pl.multiple_of((1 - core[0]) * half, half)
    for i, pack in enumerate(packs):
        to = slice(i * units, (i + 1) * units)
        gate_s[to, :] = pack[0:units, :]
        up_s[to, :] = pack[units : 2 * units, :]
        down_s[to, :] = pack[2 * units : 3 * units, pl.ds(at, half)]
    rows, far = mine[...], other[...]
    gate = mm(rows, gate_s[:, pl.ds(at, half)], NT) + mm(far, gate_s[:, pl.ds(back, half)], NT)
    up = mm(rows, up_s[:, pl.ds(at, half)], NT) + mm(far, up_s[:, pl.ds(back, half)], NT)
    out[...] = mm(clamped_unit(gate, up).astype(bf16), down_s[...])


def join_kernel(dense, mine, other, out, wide_s):
    total = (mine[...].astype(f32) + other[...].astype(f32)).astype(bf16).astype(f32)
    spread(wide_s, total, 0)
    spread(wide_s, dense[...], CAP)
    out[...] = wide_s[...].astype(bf16)


def home_kernel(home_map, returned, kept, row_gate, out, wide_s, rows_s):
    seqs, half = kept.shape
    parts = half // LANES
    peers = rows_s.shape[0] // SLOTS
    wide_s[...] = returned[...].astype(f32)
    for r in range(SLOTS):
        for c in range(parts):
            rows_s[r * peers : (r + 1) * peers, c * LANES : (c + 1) * LANES] = gather(
                wide_s, r, c, parts, peers
            )
    sums = mm(home_map[...], rows_s[...])
    out[...] = (kept[...] + sums[:seqs] + row_gate[:, 0:1] * sums[seqs:]).astype(bf16)


def swap(array):
    return lax.ppermute(array, "tp", [(0, 1), (1, 0)])


def across(array, turn):
    pairs = []
    for a in range(4):
        for b in range(4):
            for t in range(2):
                flip = (t + turn) % 2
                to = 4 * (a ^ (1 - flip)) + (b ^ flip)
                pairs.append((2 * (4 * a + b) + t, 2 * to + t))
    return lax.ppermute(array, ("ep_0", "ep_1", "tp"), pairs)


def shards(
    tokens, attn_gain, w_query1, w_query2, w_key1, w_key2, w_value, query_gain, key_gain,
    head_lambda, sub_gain, w_output, cache_key, cache_value, lengths, mix_gain, expert_gate,
    expert_up, expert_down, routes, route_weight, dense_mix, dense_gate, dense_up, dense_down,
):
    peers = lax.axis_size(EP)
    seqs, width = tokens.shape
    half, slots, wide = width // 2, CAP * peers, SLOTS * peers
    hidden = expert_gate.shape[2]
    core = lax.axis_index("tp").astype(jnp.int32).reshape(1)
    pack = jnp.concatenate([dense_gate.T, dense_up.T, dense_down], axis=0)
    pack0 = across(pack, 0)
    part, send_map, home_map = attention(
        tokens, attn_gain, w_query1, w_query2, w_key1, w_key2, w_value, query_gain,
        key_gain, head_lambda, sub_gain, w_output, cache_key, cache_value, lengths,
        routes, route_weight, peers,
    )
    block = (wide * half // LANES, LANES)
    far = swap(part)
    pack1 = across(pack, 1)
    pack2 = across(pack0, 1)
    send, kept, row_gate = call(
        mix_kernel,
        (
            core, tokens, part, far, mix_gain.reshape(1, -1),
            dense_mix.reshape(-1, LANES), send_map,
        ),
        [(block, bf16), ((seqs, half), f32), ((seqs, LANES), f32)],
        [(block, f32)],
        2 * wide * seqs * half,
    )

    def exchange(blocks):
        blocks = blocks.reshape(peers, -1, LANES)
        return lax.all_to_all(blocks, EP, 0, 0, tiled=True).reshape(block)

    mine = exchange(send)
    other = swap(mine)
    rows_mine, gate_part, up_part, gate_back, up_back = call(
        first_kernel,
        (core, mine, expert_gate, expert_up),
        [((DENSE_ROWS * peers, half), bf16)]
        + [((slots, hidden), f32)] * 2
        + [((half, hidden), bf16)] * 2,
        [(block, f32), ((slots, half), bf16)] + [((half, hidden), bf16)] * 2,
        4 * slots * half * hidden,
        far=2,
        sems=4,
    )
    rows_other, own, sent = call(
        second_kernel,
        (core, other, gate_part, up_part, gate_back, up_back, expert_down),
        [((DENSE_ROWS * peers, half), bf16)] + [((slots, half), bf16)] * 2,
        [(block, f32), ((slots, half), bf16), ((slots, width), f32)],
        8 * slots * half * hidden,
        slots * hidden,
    )
    came = swap(sent)
    packs = [pack, pack0, pack1, pack2]
    packs = packs + [swap(one) for one in packs]
    units = pack.shape[0] // 3 * len(packs)
    (dense,) = call(
        dense_kernel,
        (core, rows_mine, rows_other, *packs),
        [((DENSE_ROWS * peers, half), f32)],
        [((units, width), bf16), ((units, width), bf16), ((units, half), bf16)],
        10 * DENSE_ROWS * peers * half * units,
        DENSE_ROWS * peers * units,
    )
    (joined,) = call(join_kernel, (dense, own, came), [(block, bf16)], [(block, f32)], 0)
    returned = exchange(joined)
    (out,) = call(
        home_kernel,
        (home_map, returned, kept, row_gate),
        [((seqs, half), bf16)],
        [(block, f32), ((wide, half), bf16)],
        4 * seqs * wide * half,
    )
    return out


def solution(mesh):
    torus = Mesh(mesh.devices.reshape(4, 4, 4, mesh.shape["tp"]), EP_TP)
    in_specs = (
        P(EP, None), P(), P(None, "tp"), P(None, "tp"), P(None, "tp"), P(None, "tp"),
        P(None, "tp"), P(), P(), P("tp"), P(), P("tp", None), P(EP, "tp", None, None),
        P(EP, "tp", None, None), P(EP), P(), P(EP, None, "tp"), P(EP, None, "tp"),
        P(EP, "tp", None), P(EP, None), P(EP, None), P(), P(None, EP_TP), P(None, EP_TP),
        P(EP_TP, None),
    )
    return jax.shard_map(
        shards, mesh=torus, in_specs=in_specs, out_specs=P(EP, "tp"), check_vma=False
    )
```

```python
import functools

import jax
import jax.numpy as jnp
from jax import lax
from jax.experimental import pallas as pl
from jax.experimental.pallas import tpu as pltpu
from jax.sharding import Mesh
from jax.sharding import PartitionSpec as P


HEAD = 64
VHEAD = 128
EP = ("ep_0", "ep_1", "ep_2")
EP_TP = ("ep_0", "ep_1", "ep_2", "tp")
SLOTS = 6
CAP = 2
DENSE_ROWS = 4
LANES = 128
SEQ_STEP = 8
LIMIT = 40 << 20

epsilon = 1e-05
clamp_limit = 7.0
sigmoid_slope = 1.702
lambda_start = 0.2
neg_large = -1e30

bf16 = jnp.bfloat16
f32 = jnp.float32
NT = (((1,), (1,)), ((), ()))
TN = (((0,), (0,)), ((), ()))


def mm(a, b, dims=(((1,), (0,)), ((), ()))):
    return lax.dot_general(a, b, dims, preferred_element_type=f32)


def clamped_unit(gate_pre, up_pre):
    gate_pre = jnp.minimum(gate_pre, clamp_limit)
    up_pre = jnp.clip(up_pre, -clamp_limit, clamp_limit)
    return gate_pre * jax.nn.sigmoid(sigmoid_slope * gate_pre) * (up_pre + 1.0)


def rms(values):
    return lax.rsqrt(jnp.mean(values * values, axis=-1, keepdims=True) + epsilon)


def routing_maps(routes_t, weight_t, seqs, peers):
    wide = peers * SLOTS
    diag = lax.broadcasted_iota(jnp.int32, (seqs, seqs), 0) == lax.broadcasted_iota(
        jnp.int32, (seqs, seqs), 1
    )
    lane = lax.broadcasted_iota(jnp.int32, (seqs, wide), 1)
    peer, slot = lane % peers, lane // peers
    token = lax.broadcasted_iota(jnp.int32, (seqs, wide), 0)
    hit = jnp.zeros((seqs, wide), f32)
    weight = jnp.zeros((seqs, wide), f32)
    for k in range(routes_t.shape[0]):
        expert = jnp.sum(
            jnp.where(diag, routes_t[k : k + 1, :].astype(f32), 0.0), axis=1, keepdims=True
        ).astype(jnp.int32)
        share = jnp.sum(
            jnp.where(diag, weight_t[k : k + 1, :].astype(f32), 0.0), axis=1, keepdims=True
        )
        same = peer == expert
        hit = jnp.where(same, 1.0, hit)
        weight = jnp.where(same, share, weight)
    before = (
        lax.broadcasted_iota(jnp.int32, (seqs, seqs), 1)
        < lax.broadcasted_iota(jnp.int32, (seqs, seqs), 0)
    ).astype(bf16)
    rank = mm(before, hit.astype(bf16))
    chosen = (hit > 0.0) & (rank == slot.astype(f32)) & (slot < CAP)
    group = 2 * ((peer // 16) % 2) + (peer // 4) % 2
    dense = (token == group * DENSE_ROWS + slot - CAP) & (slot >= CAP)
    return (
        jnp.where(chosen | dense, 1.0, 0.0).astype(bf16),
        jnp.where(chosen, weight, 0.0).astype(bf16),
        jnp.where(dense, 1.0, 0.0).astype(bf16),
    )


def attention_kernel(*refs, peers):
    sources, refs = refs[:17], refs[17:]
    part, send_map, home_map = refs[:3]
    query_s, key_s, value_s, heads_s, *local = refs[3:-1]
    sems = refs[-1]
    (
        lengths, lam, tokens, attn_gain, w_query1, w_query2, w_key1, w_key2, w_value, query_gain, key_gain,
        routes_t, weight_t, sub_gain, w_output, cache_key, cache_value,
    ) = local
    seqs = tokens.shape[0]
    heads = w_query1.shape[1] // HEAD
    cached = cache_key.shape[2]
    rounds = seqs // SEQ_STEP
    copies = [
        pltpu.make_async_copy(sources[i], local[i], sems.at[i]) for i in range(len(local) - 2)
    ]
    chunks = []
    for b in range(rounds):
        of = pl.ds(b * SEQ_STEP, SEQ_STEP)
        for j in (0, 1):
            at = len(copies) + len(chunks)
            source, to = sources[15 + j].at[of], local[15 + j].at[of]
            chunks.append(pltpu.make_async_copy(source, to, sems.at[at]))
    for one in copies[:-1] + chunks + copies[-1:]:
        one.start()

    for one in copies[:-1]:
        one.wait()
    rows = tokens[...].astype(f32)
    normed = (rows * rms(rows) * attn_gain[...]).astype(bf16)
    nothing = jnp.zeros((seqs, HEAD), f32)
    for m, weight in enumerate((w_query1, w_query2)):
        query = mm(normed, weight[...])
        for h in range(heads):
            one = query[:, h * HEAD : (h + 1) * HEAD]
            one = (one * rms(one) * query_gain[...]).astype(bf16).astype(f32) * HEAD**-0.5
            pair = (one, nothing) if m == 0 else (nothing, one)
            at = (m * heads + h) * seqs
            query_s[at : at + seqs, :] = jnp.concatenate(pair, axis=1)
    new_keys = []
    for weight in (w_key1, w_key2):
        one = mm(normed, weight[...], NT)
        new_keys.append((one * rms(one) * key_gain[...]).astype(bf16).astype(f32))
    key_s[...] = jnp.concatenate(new_keys, axis=1)
    value_s[...] = mm(normed, w_value[...]).astype(bf16).astype(f32)
    send, routed, dense = routing_maps(routes_t[...], weight_t[...], seqs, peers)
    send_map[...] = send
    home_map[0:seqs, :] = routed
    home_map[seqs : 2 * seqs, :] = dense

    row = lax.broadcasted_iota(jnp.int32, (2 * heads, 1), 0)
    signed = jnp.ones((2 * heads, 1), f32)
    for h in range(heads):
        signed = jnp.where(row == heads + h, -lam[h], signed)
    lane = lax.broadcasted_iota(jnp.int32, (2 * heads, cached), 1)
    for b in range(rounds):
        span = range(b * SEQ_STEP, (b + 1) * SEQ_STEP)
        chunks[2 * b].wait()
        queries = [query_s[pl.ds(s, 2 * heads, stride=seqs), :] for s in span]
        fresh = [
            jnp.sum(query * key_s[s : s + 1, :], axis=1, keepdims=True)
            for s, query in zip(span, queries)
        ]
        scores = [
            jnp.where(lane < lengths[s], mm(query.astype(bf16), cache_key[s, 0], NT), neg_large)
            for s, query in zip(span, queries)
        ]
        top = [
            jnp.maximum(jnp.max(one, axis=1, keepdims=True), new)
            for one, new in zip(scores, fresh)
        ]
        expo = [jnp.exp(one - most) for one, most in zip(scores, top)]
        fresh_expo = [jnp.exp(one - most) for one, most in zip(fresh, top)]
        scale = [
            signed / (jnp.sum(one, axis=1, keepdims=True) + new)
            for one, new in zip(expo, fresh_expo)
        ]
        probs = [one * by for one, by in zip(expo, scale)]
        probs = [(one + pltpu.roll(one, heads, 0)).astype(bf16) for one in probs]
        chunks[2 * b + 1].wait()
        for s, one, new, by in zip(span, probs, fresh_expo, scale):
            new = new * by
            new = (new[0:heads] + new[heads:]).astype(bf16).astype(f32)
            heads_out = mm(one, cache_value[s, 0])[0:heads] + new * value_s[s : s + 1, :]
            heads_s[pl.ds(s, heads, stride=seqs), :] = heads_out

    subs = []
    for h in range(heads):
        one = heads_s[h * seqs : (h + 1) * seqs, :]
        subs.append((one * rms(one) * sub_gain[...] * (1.0 - lambda_start)).astype(bf16))
    copies[-1].wait()
    part[...] = mm(jnp.concatenate(subs, axis=1), w_output[...]).astype(bf16)


def attention(
    tokens, attn_gain, w_query1, w_query2, w_key1, w_key2, w_value, query_gain, key_gain,
    head_lambda, sub_gain, w_output, cache_key, cache_value, lengths, routes, route_weight,
    peers,
):
    seqs, width = tokens.shape
    heads = w_query1.shape[1] // HEAD
    cached = cache_key.shape[2]
    local = [
        lengths, head_lambda, tokens, attn_gain.reshape(1, -1), w_query1, w_query2, w_key1.T, w_key2.T, w_value,
        query_gain.reshape(1, -1), key_gain.reshape(1, -1), routes.T, route_weight.T,
        sub_gain.reshape(1, -1), w_output, cache_key, cache_value,
    ]
    flops = 2 * seqs * width * (2 * heads * HEAD + 2 * HEAD + VHEAD + heads * VHEAD)
    flops += 6 * seqs * 8 * cached * VHEAD
    wide = peers * SLOTS
    count = len(local) - 2 + 2 * (seqs // SEQ_STEP)
    return pl.pallas_call(
        functools.partial(attention_kernel, peers=peers),
        in_specs=[pl.BlockSpec(memory_space=pltpu.HBM)] * len(local),
        out_specs=[pl.BlockSpec(memory_space=pltpu.VMEM)] * 3,
        out_shape=[
            pltpu.VMEM((seqs, width), bf16),
            pltpu.VMEM((seqs, wide), bf16),
            pltpu.VMEM((2 * seqs, wide), bf16),
        ],
        scratch_shapes=[
            pltpu.VMEM((2 * heads * seqs, 2 * HEAD), f32),
            pltpu.VMEM((seqs, 2 * HEAD), f32),
            pltpu.VMEM((seqs, VHEAD), f32),
            pltpu.VMEM((heads * seqs, VHEAD), f32),
        ]
        + [pltpu.SMEM(one.shape, one.dtype) for one in local[:2]]
        + [pltpu.VMEM(one.shape, one.dtype) for one in local[2:]]
        + [pltpu.SemaphoreType.DMA((count,))],
        compiler_params=pltpu.CompilerParams(vmem_limit_bytes=LIMIT),
        cost_estimate=pl.CostEstimate(
            flops=flops, bytes_accessed=13 << 20, transcendentals=seqs * 8 * cached
        ),
        name="attention",
    )(*[pltpu.with_memory_space_constraint(one, pltpu.HBM) for one in local])


def spread(wide_s, rows, first):
    slots, peers, parts = wide_s.shape[0] // 64 // 8, 64, rows.shape[1] // LANES
    for r in range(rows.shape[0] // peers):
        for c in range(parts):
            wide_s[pl.ds((first + r) * parts + c, peers, stride=slots * parts), :] = rows[
                r * peers : (r + 1) * peers, c * LANES : (c + 1) * LANES
            ]


def gather(wide_s, r, c, parts, peers):
    slots = wide_s.shape[0] // peers // parts
    return wide_s[pl.ds(r * parts + c, peers, stride=slots * parts), :].astype(bf16)


def mix_kernel(tokens, mine, other, mix_gain, dense_mix, send_map, send, kept, row_gate, wide_s):
    half = kept.shape[1]
    attn_out = mine[...].astype(f32) + other[...].astype(f32)
    residual = (tokens[...].astype(f32) + attn_out).astype(bf16)
    rows = residual.astype(f32)
    mixed = (rows * rms(rows) * mix_gain[...]).astype(bf16).astype(f32)
    first = lax.axis_index("tp") == 0
    kept[...] = jnp.where(first, rows[:, :half], rows[:, half:])
    gate = jnp.zeros((rows.shape[0], LANES), f32)
    for c in range(rows.shape[1] // LANES):
        gate = gate + mixed[:, c * LANES : (c + 1) * LANES] * dense_mix[c : c + 1, :].astype(f32)
    gate = jnp.sum(gate, axis=1, keepdims=True)
    row_gate[...] = jnp.broadcast_to(jax.nn.sigmoid(gate), row_gate.shape)
    columns = jnp.where(first, mixed[:, :half], mixed[:, half:]).astype(bf16)
    spread(wide_s, mm(send_map[...], columns, TN), 0)
    send[...] = wide_s[...].astype(bf16)


def call(kernel, args, outs, scratch, flops, transcendentals=0, far=0, sems=0):
    near = len(args) - far
    spaces = [pltpu.SMEM if one.ndim == 1 else pltpu.VMEM for one in args[:near]]
    spaces += [pltpu.HBM] * far
    args = list(args[:near]) + [
        pltpu.with_memory_space_constraint(one, pltpu.HBM) for one in args[near:]
    ]
    out_shape = [jax.ShapeDtypeStruct(*one) for one in outs]
    moved = sum(one.size * one.dtype.itemsize for one in args + out_shape)
    return pl.pallas_call(
        kernel,
        in_specs=[pl.BlockSpec(memory_space=space) for space in spaces],
        out_specs=[pl.BlockSpec(memory_space=pltpu.VMEM)] * len(outs),
        out_shape=out_shape,
        scratch_shapes=[pltpu.VMEM(*one) for one in scratch]
        + [pltpu.SemaphoreType.DMA((sems,))] * (sems > 0),
        compiler_params=pltpu.CompilerParams(vmem_limit_bytes=LIMIT // 2),
        cost_estimate=pl.CostEstimate(
            flops=flops, bytes_accessed=moved, transcendentals=transcendentals
        ),
    )(*args)


def compact(wide_s, rows_e, rows_d):
    parts, peers = rows_d.shape[1] // LANES, rows_e.shape[0] // CAP
    for r in range(SLOTS):
        for c in range(parts):
            to, at = (rows_e, r) if r < CAP else (rows_d, r - CAP)
            to[at * peers : (at + 1) * peers, c * LANES : (c + 1) * LANES] = gather(
                wide_s, r, c, parts, peers
            )


def first_kernel(
    mine, gate, up, rows_d, gate_part, up_part, wide_s, rows_e,
):
    half = rows_d.shape[1]
    own = pl.ds(pl.multiple_of(lax.axis_index("tp") * half, half), half)
    wide_s[...] = mine[...].astype(f32)
    compact(wide_s, rows_e, rows_d)
    gate_part[...] = mm(rows_e[...], gate[0, own])
    up_part[...] = mm(rows_e[...], up[0, own])


def second_kernel(
    other, gate_part, up_part, gate, up, down, rows_d, out_mine, out_other,
    wide_s, rows_e, total,
):
    half = rows_d.shape[1]
    at = pl.multiple_of(lax.axis_index("tp") * half, half)
    back = pl.multiple_of((1 - lax.axis_index("tp")) * half, half)
    wide_s[...] = other[...].astype(f32)
    compact(wide_s, rows_e, rows_d)
    gate_pre = gate_part[...] + mm(rows_e[...], gate[0, pl.ds(back, half)])
    up_pre = up_part[...] + mm(rows_e[...], up[0, pl.ds(back, half)])
    hidden = clamped_unit(gate_pre, up_pre).astype(bf16)
    total[...] = mm(hidden, down[0])
    out_mine[...] = total[:, pl.ds(at, half)].astype(bf16)
    out_other[...] = total[:, pl.ds(back, half)].astype(bf16)


def dense_kernel(mine, other, *refs):
    packs, out, gate_s, up_s, down_s = refs[:-4], refs[-4], refs[-3], refs[-2], refs[-1]
    half = mine.shape[1]
    units = packs[0].shape[0] // 3
    at = pl.multiple_of(lax.axis_index("tp") * half, half)
    back = pl.multiple_of((1 - lax.axis_index("tp")) * half, half)
    for i, pack in enumerate(packs):
        to = slice(i * units, (i + 1) * units)
        gate_s[to, :] = pack[0:units, :]
        up_s[to, :] = pack[units : 2 * units, :]
        down_s[to, :] = pack[2 * units : 3 * units, pl.ds(at, half)]
    rows, far = mine[...], other[...]
    gate = mm(rows, gate_s[:, pl.ds(at, half)], NT) + mm(far, gate_s[:, pl.ds(back, half)], NT)
    up = mm(rows, up_s[:, pl.ds(at, half)], NT) + mm(far, up_s[:, pl.ds(back, half)], NT)
    out[...] = mm(clamped_unit(gate, up).astype(bf16), down_s[...])


def join_kernel(dense, mine, other, out, wide_s):
    total = (mine[...].astype(f32) + other[...].astype(f32)).astype(bf16).astype(f32)
    spread(wide_s, total, 0)
    spread(wide_s, dense[...], CAP)
    out[...] = wide_s[...].astype(bf16)


def home_kernel(home_map, returned, kept, row_gate, out, wide_s, rows_s):
    seqs, half = kept.shape
    parts = half // LANES
    peers = rows_s.shape[0] // SLOTS
    wide_s[...] = returned[...].astype(f32)
    for r in range(SLOTS):
        for c in range(parts):
            rows_s[r * peers : (r + 1) * peers, c * LANES : (c + 1) * LANES] = gather(
                wide_s, r, c, parts, peers
            )
    sums = mm(home_map[...], rows_s[...])
    out[...] = (kept[...] + sums[:seqs] + row_gate[:, 0:1] * sums[seqs:]).astype(bf16)


def swap(array):
    return lax.ppermute(array, "tp", [(0, 1), (1, 0)])


def across(array, turn):
    pairs = []
    for a in range(4):
        for b in range(4):
            for t in range(2):
                flip = (t + turn) % 2
                to = 4 * (a ^ (1 - flip)) + (b ^ flip)
                pairs.append((2 * (4 * a + b) + t, 2 * to + t))
    return lax.ppermute(array, ("ep_0", "ep_1", "tp"), pairs)


def shards(
    tokens, attn_gain, w_query1, w_query2, w_key1, w_key2, w_value, query_gain, key_gain,
    head_lambda, sub_gain, w_output, cache_key, cache_value, lengths, mix_gain, expert_gate,
    expert_up, expert_down, routes, route_weight, dense_mix, dense_gate, dense_up, dense_down,
):
    peers = lax.axis_size(EP)
    seqs, width = tokens.shape
    half, slots, wide = width // 2, CAP * peers, SLOTS * peers
    hidden = expert_gate.shape[2]
    pack = jnp.concatenate([dense_gate.T, dense_up.T, dense_down], axis=0)
    pack0 = across(pack, 0)
    part, send_map, home_map = attention(
        tokens, attn_gain, w_query1, w_query2, w_key1, w_key2, w_value, query_gain,
        key_gain, head_lambda, sub_gain, w_output, cache_key, cache_value, lengths,
        routes, route_weight, peers,
    )
    block = (wide * half // LANES, LANES)
    far = swap(part)
    pack1 = across(pack, 1)
    pack2 = across(pack0, 1)
    send, kept, row_gate = call(
        mix_kernel,
        (
            tokens, part, far, mix_gain.reshape(1, -1),
            dense_mix.reshape(-1, LANES), send_map,
        ),
        [(block, bf16), ((seqs, half), f32), ((seqs, LANES), f32)],
        [(block, f32)],
        2 * wide * seqs * half,
    )

    def exchange(blocks):
        blocks = blocks.reshape(peers, -1, LANES)
        return lax.all_to_all(blocks, EP, 0, 0, tiled=True).reshape(block)

    mine = exchange(send)
    other = swap(mine)
    rows_mine, gate_part, up_part = call(
        first_kernel,
        (mine, expert_gate, expert_up),
        [((DENSE_ROWS * peers, half), bf16)] + [((slots, hidden), f32)] * 2,
        [(block, f32), ((slots, half), bf16)],
        4 * slots * half * hidden,
    )
    rows_other, own, sent = call(
        second_kernel,
        (other, gate_part, up_part, expert_gate, expert_up, expert_down),
        [((DENSE_ROWS * peers, half), bf16)] + [((slots, half), bf16)] * 2,
        [(block, f32), ((slots, half), bf16), ((slots, width), f32)],
        8 * slots * half * hidden,
        slots * hidden,
    )
    came = swap(sent)
    packs = [pack, pack0, pack1, pack2]
    packs = packs + [swap(one) for one in packs]
    units = pack.shape[0] // 3 * len(packs)
    (dense,) = call(
        dense_kernel,
        (rows_mine, rows_other, *packs),
        [((DENSE_ROWS * peers, half), f32)],
        [((units, width), bf16), ((units, width), bf16), ((units, half), bf16)],
        10 * DENSE_ROWS * peers * half * units,
        DENSE_ROWS * peers * units,
    )
    (joined,) = call(join_kernel, (dense, own, came), [(block, bf16)], [(block, f32)], 0)
    returned = exchange(joined)
    (out,) = call(
        home_kernel,
        (home_map, returned, kept, row_gate),
        [((seqs, half), bf16)],
        [(block, f32), ((wide, half), bf16)],
        4 * seqs * wide * half,
    )
    return out


def solution(mesh):
    torus = Mesh(mesh.devices.reshape(4, 4, 4, mesh.shape["tp"]), EP_TP)
    in_specs = (
        P(EP, None), P(), P(None, "tp"), P(None, "tp"), P(None, "tp"), P(None, "tp"),
        P(None, "tp"), P(), P(), P("tp"), P(), P("tp", None), P(EP, "tp", None, None),
        P(EP, "tp", None, None), P(EP), P(), P(EP, None, "tp"), P(EP, None, "tp"),
        P(EP, "tp", None), P(EP, None), P(EP, None), P(), P(None, EP_TP), P(None, EP_TP),
        P(EP_TP, None),
    )
    return jax.shard_map(
        shards, mesh=torus, in_specs=in_specs, out_specs=P(EP, "tp"), check_vma=False
    )
```

```python
import functools

import jax
import jax.numpy as jnp
from jax import lax
from jax.experimental import pallas as pl
from jax.experimental.pallas import tpu as pltpu
from jax.sharding import Mesh
from jax.sharding import PartitionSpec as P


HEAD = 64
VHEAD = 128
EP = ("ep_0", "ep_1", "ep_2")
EP_TP = ("ep_0", "ep_1", "ep_2", "tp")
SLOTS = 6
CAP = 2
DENSE_ROWS = 4
LANES = 128
SEQ_STEP = 8
LIMIT = 40 << 20

epsilon = 1e-05
clamp_limit = 7.0
sigmoid_slope = 1.702
lambda_start = 0.2
neg_large = -1e30

bf16 = jnp.bfloat16
f32 = jnp.float32
NT = (((1,), (1,)), ((), ()))
TN = (((0,), (0,)), ((), ()))


def mm(a, b, dims=(((1,), (0,)), ((), ()))):
    return lax.dot_general(a, b, dims, preferred_element_type=f32)


def clamped_unit(gate_pre, up_pre):
    gate_pre = jnp.minimum(gate_pre, clamp_limit)
    up_pre = jnp.clip(up_pre, -clamp_limit, clamp_limit)
    return gate_pre * jax.nn.sigmoid(sigmoid_slope * gate_pre) * (up_pre + 1.0)


def rms(values):
    return lax.rsqrt(jnp.mean(values * values, axis=-1, keepdims=True) + epsilon)


def routing_maps(routes_t, weight_t, seqs, peers):
    wide = peers * SLOTS
    diag = lax.broadcasted_iota(jnp.int32, (seqs, seqs), 0) == lax.broadcasted_iota(
        jnp.int32, (seqs, seqs), 1
    )
    lane = lax.broadcasted_iota(jnp.int32, (seqs, wide), 1)
    peer, slot = lane % peers, lane // peers
    token = lax.broadcasted_iota(jnp.int32, (seqs, wide), 0)
    hit = jnp.zeros((seqs, wide), f32)
    weight = jnp.zeros((seqs, wide), f32)
    for k in range(routes_t.shape[0]):
        expert = jnp.sum(
            jnp.where(diag, routes_t[k : k + 1, :].astype(f32), 0.0), axis=1, keepdims=True
        ).astype(jnp.int32)
        share = jnp.sum(
            jnp.where(diag, weight_t[k : k + 1, :].astype(f32), 0.0), axis=1, keepdims=True
        )
        same = peer == expert
        hit = jnp.where(same, 1.0, hit)
        weight = jnp.where(same, share, weight)
    before = (
        lax.broadcasted_iota(jnp.int32, (seqs, seqs), 1)
        < lax.broadcasted_iota(jnp.int32, (seqs, seqs), 0)
    ).astype(bf16)
    rank = mm(before, hit.astype(bf16))
    chosen = (hit > 0.0) & (rank == slot.astype(f32)) & (slot < CAP)
    group = 2 * ((peer // 16) % 2) + (peer // 4) % 2
    dense = (token == group * DENSE_ROWS + slot - CAP) & (slot >= CAP)
    return (
        jnp.where(chosen | dense, 1.0, 0.0).astype(bf16),
        jnp.where(chosen, weight, 0.0).astype(bf16),
        jnp.where(dense, 1.0, 0.0).astype(bf16),
    )


def attention_kernel(*refs, peers):
    w_query1, w_query2, w_key1, w_key2, w_value, w_output = refs[:6]
    sources, refs = refs[6:17], refs[17:]
    part, send_map, home_map = refs[:3]
    query_s, key_s, value_s, heads_s, *local = refs[3:-1]
    sems = refs[-1]
    (
        lengths, lam, tokens, attn_gain, query_gain, key_gain, routes_t, weight_t, sub_gain,
        cache_key, cache_value,
    ) = local
    seqs = tokens.shape[0]
    heads = w_query1.shape[1] // HEAD
    cached = cache_key.shape[2]
    rounds = seqs // SEQ_STEP
    copies = [
        pltpu.make_async_copy(sources[i], local[i], sems.at[i]) for i in range(len(local) - 2)
    ]
    chunks = []
    for b in range(rounds):
        of = pl.ds(b * SEQ_STEP, SEQ_STEP)
        for j in (0, 1):
            at = len(copies) + len(chunks)
            source, to = sources[9 + j].at[of], local[9 + j].at[of]
            chunks.append(pltpu.make_async_copy(source, to, sems.at[at]))
    for one in copies + chunks:
        one.start()

    for one in copies:
        one.wait()
    rows = tokens[...].astype(f32)
    normed = (rows * rms(rows) * attn_gain[...]).astype(bf16)
    nothing = jnp.zeros((seqs, HEAD), f32)
    for m, weight in enumerate((w_query1, w_query2)):
        query = mm(normed, weight[...])
        for h in range(heads):
            one = query[:, h * HEAD : (h + 1) * HEAD]
            one = (one * rms(one) * query_gain[...]).astype(bf16).astype(f32) * HEAD**-0.5
            pair = (one, nothing) if m == 0 else (nothing, one)
            at = (m * heads + h) * seqs
            query_s[at : at + seqs, :] = jnp.concatenate(pair, axis=1)
    new_keys = []
    for weight in (w_key1, w_key2):
        one = mm(normed, weight[...], NT)
        new_keys.append((one * rms(one) * key_gain[...]).astype(bf16).astype(f32))
    key_s[...] = jnp.concatenate(new_keys, axis=1)
    value_s[...] = mm(normed, w_value[...]).astype(bf16).astype(f32)
    send, routed, dense = routing_maps(routes_t[...], weight_t[...], seqs, peers)
    send_map[...] = send
    home_map[0:seqs, :] = routed
    home_map[seqs : 2 * seqs, :] = dense

    row = lax.broadcasted_iota(jnp.int32, (2 * heads, 1), 0)
    signed = jnp.ones((2 * heads, 1), f32)
    for h in range(heads):
        signed = jnp.where(row == heads + h, -lam[h], signed)
    lane = lax.broadcasted_iota(jnp.int32, (2 * heads, cached), 1)
    for b in range(rounds):
        span = range(b * SEQ_STEP, (b + 1) * SEQ_STEP)
        chunks[2 * b].wait()
        queries = [query_s[pl.ds(s, 2 * heads, stride=seqs), :] for s in span]
        fresh = [
            jnp.sum(query * key_s[s : s + 1, :], axis=1, keepdims=True)
            for s, query in zip(span, queries)
        ]
        scores = [
            jnp.where(lane < lengths[s], mm(query.astype(bf16), cache_key[s, 0], NT), neg_large)
            for s, query in zip(span, queries)
        ]
        top = [
            jnp.maximum(jnp.max(one, axis=1, keepdims=True), new)
            for one, new in zip(scores, fresh)
        ]
        expo = [jnp.exp(one - most) for one, most in zip(scores, top)]
        fresh_expo = [jnp.exp(one - most) for one, most in zip(fresh, top)]
        scale = [
            signed / (jnp.sum(one, axis=1, keepdims=True) + new)
            for one, new in zip(expo, fresh_expo)
        ]
        probs = [one * by for one, by in zip(expo, scale)]
        probs = [(one + pltpu.roll(one, heads, 0)).astype(bf16) for one in probs]
        chunks[2 * b + 1].wait()
        for s, one, new, by in zip(span, probs, fresh_expo, scale):
            new = new * by
            new = (new[0:heads] + new[heads:]).astype(bf16).astype(f32)
            heads_out = mm(one, cache_value[s, 0])[0:heads] + new * value_s[s : s + 1, :]
            heads_s[pl.ds(s, heads, stride=seqs), :] = heads_out

    subs = []
    for h in range(heads):
        one = heads_s[h * seqs : (h + 1) * seqs, :]
        subs.append((one * rms(one) * sub_gain[...] * (1.0 - lambda_start)).astype(bf16))
    part[...] = mm(jnp.concatenate(subs, axis=1), w_output[...]).astype(bf16)


def attention(
    tokens, attn_gain, w_query1, w_query2, w_key1, w_key2, w_value, query_gain, key_gain,
    head_lambda, sub_gain, w_output, cache_key, cache_value, lengths, routes, route_weight,
    peers,
):
    seqs, width = tokens.shape
    heads = w_query1.shape[1] // HEAD
    cached = cache_key.shape[2]
    local = [
        lengths, head_lambda, tokens, attn_gain.reshape(1, -1), query_gain.reshape(1, -1),
        key_gain.reshape(1, -1), routes.T, route_weight.T, sub_gain.reshape(1, -1), cache_key,
        cache_value,
    ]
    near = [w_query1, w_query2, w_key1.T, w_key2.T, w_value, w_output]
    flops = 2 * seqs * width * (2 * heads * HEAD + 2 * HEAD + VHEAD + heads * VHEAD)
    flops += 6 * seqs * 8 * cached * VHEAD
    wide = peers * SLOTS
    count = len(local) - 2 + 2 * (seqs // SEQ_STEP)
    return pl.pallas_call(
        functools.partial(attention_kernel, peers=peers),
        in_specs=[pl.BlockSpec(memory_space=pltpu.VMEM)] * len(near)
        + [pl.BlockSpec(memory_space=pltpu.HBM)] * len(local),
        out_specs=[pl.BlockSpec(memory_space=pltpu.VMEM)] * 3,
        out_shape=[
            pltpu.VMEM((seqs, width), bf16),
            pltpu.VMEM((seqs, wide), bf16),
            pltpu.VMEM((2 * seqs, wide), bf16),
        ],
        scratch_shapes=[
            pltpu.VMEM((2 * heads * seqs, 2 * HEAD), f32),
            pltpu.VMEM((seqs, 2 * HEAD), f32),
            pltpu.VMEM((seqs, VHEAD), f32),
            pltpu.VMEM((heads * seqs, VHEAD), f32),
        ]
        + [pltpu.SMEM(one.shape, one.dtype) for one in local[:2]]
        + [pltpu.VMEM(one.shape, one.dtype) for one in local[2:]]
        + [pltpu.SemaphoreType.DMA((count,))],
        compiler_params=pltpu.CompilerParams(vmem_limit_bytes=LIMIT),
        cost_estimate=pl.CostEstimate(
            flops=flops, bytes_accessed=13 << 20, transcendentals=seqs * 8 * cached
        ),
        name="attention",
    )(*near, *[pltpu.with_memory_space_constraint(one, pltpu.HBM) for one in local])


def spread(wide_s, rows, first):
    slots, peers, parts = wide_s.shape[0] // 64 // 8, 64, rows.shape[1] // LANES
    for r in range(rows.shape[0] // peers):
        for c in range(parts):
            wide_s[pl.ds((first + r) * parts + c, peers, stride=slots * parts), :] = rows[
                r * peers : (r + 1) * peers, c * LANES : (c + 1) * LANES
            ]


def gather(wide_s, r, c, parts, peers):
    slots = wide_s.shape[0] // peers // parts
    return wide_s[pl.ds(r * parts + c, peers, stride=slots * parts), :].astype(bf16)


def mix_kernel(tokens, mine, other, mix_gain, dense_mix, send_map, send, kept, row_gate, wide_s):
    half = kept.shape[1]
    attn_out = mine[...].astype(f32) + other[...].astype(f32)
    residual = (tokens[...].astype(f32) + attn_out).astype(bf16)
    rows = residual.astype(f32)
    mixed = (rows * rms(rows) * mix_gain[...]).astype(bf16).astype(f32)
    first = lax.axis_index("tp") == 0
    kept[...] = jnp.where(first, rows[:, :half], rows[:, half:])
    gate = jnp.zeros((rows.shape[0], LANES), f32)
    for c in range(rows.shape[1] // LANES):
        gate = gate + mixed[:, c * LANES : (c + 1) * LANES] * dense_mix[c : c + 1, :].astype(f32)
    gate = jnp.sum(gate, axis=1, keepdims=True)
    row_gate[...] = jnp.broadcast_to(jax.nn.sigmoid(gate), row_gate.shape)
    columns = jnp.where(first, mixed[:, :half], mixed[:, half:]).astype(bf16)
    spread(wide_s, mm(send_map[...], columns, TN), 0)
    send[...] = wide_s[...].astype(bf16)


def call(kernel, args, outs, scratch, flops, transcendentals=0, far=0, sems=0):
    near = len(args) - far
    spaces = [pltpu.SMEM if one.ndim == 1 else pltpu.VMEM for one in args[:near]]
    spaces += [pltpu.HBM] * far
    args = list(args[:near]) + [
        pltpu.with_memory_space_constraint(one, pltpu.HBM) for one in args[near:]
    ]
    out_shape = [jax.ShapeDtypeStruct(*one) for one in outs]
    moved = sum(one.size * one.dtype.itemsize for one in args + out_shape)
    return pl.pallas_call(
        kernel,
        in_specs=[pl.BlockSpec(memory_space=space) for space in spaces],
        out_specs=[pl.BlockSpec(memory_space=pltpu.VMEM)] * len(outs),
        out_shape=out_shape,
        scratch_shapes=[pltpu.VMEM(*one) for one in scratch]
        + [pltpu.SemaphoreType.DMA((sems,))] * (sems > 0),
        compiler_params=pltpu.CompilerParams(vmem_limit_bytes=LIMIT // 2),
        cost_estimate=pl.CostEstimate(
            flops=flops, bytes_accessed=moved, transcendentals=transcendentals
        ),
    )(*args)


def compact(wide_s, rows_e, rows_d):
    parts, peers = rows_d.shape[1] // LANES, rows_e.shape[0] // CAP
    for r in range(SLOTS):
        for c in range(parts):
            to, at = (rows_e, r) if r < CAP else (rows_d, r - CAP)
            to[at * peers : (at + 1) * peers, c * LANES : (c + 1) * LANES] = gather(
                wide_s, r, c, parts, peers
            )


def first_kernel(
    mine, gate, up, rows_d, gate_part, up_part, wide_s, rows_e,
):
    half = rows_d.shape[1]
    own = pl.ds(pl.multiple_of(lax.axis_index("tp") * half, half), half)
    wide_s[...] = mine[...].astype(f32)
    compact(wide_s, rows_e, rows_d)
    gate_part[...] = mm(rows_e[...], gate[0, own])
    up_part[...] = mm(rows_e[...], up[0, own])


def second_kernel(
    other, gate_part, up_part, gate, up, down, rows_d, out_mine, out_other,
    wide_s, rows_e, total,
):
    half = rows_d.shape[1]
    at = pl.multiple_of(lax.axis_index("tp") * half, half)
    back = pl.multiple_of((1 - lax.axis_index("tp")) * half, half)
    wide_s[...] = other[...].astype(f32)
    compact(wide_s, rows_e, rows_d)
    gate_pre = gate_part[...] + mm(rows_e[...], gate[0, pl.ds(back, half)])
    up_pre = up_part[...] + mm(rows_e[...], up[0, pl.ds(back, half)])
    hidden = clamped_unit(gate_pre, up_pre).astype(bf16)
    total[...] = mm(hidden, down[0])
    out_mine[...] = total[:, pl.ds(at, half)].astype(bf16)
    out_other[...] = total[:, pl.ds(back, half)].astype(bf16)


def pack_kernel(gate, up, down, out, sems):
    units = gate.shape[0]
    copies = [
        pltpu.make_async_copy(one, out.at[pl.ds(i * units, units)], sems.at[i])
        for i, one in enumerate((gate, up, down))
    ]
    for one in copies:
        one.start()
    for one in copies:
        one.wait()


def dense_kernel(mine, other, *refs):
    packs, out, gate_s, up_s, down_s = refs[:-4], refs[-4], refs[-3], refs[-2], refs[-1]
    half = mine.shape[1]
    units = packs[0].shape[0] // 3
    at = pl.multiple_of(lax.axis_index("tp") * half, half)
    back = pl.multiple_of((1 - lax.axis_index("tp")) * half, half)
    for i, pack in enumerate(packs):
        to = slice(i * units, (i + 1) * units)
        gate_s[to, :] = pack[0:units, :]
        up_s[to, :] = pack[units : 2 * units, :]
        down_s[to, :] = pack[2 * units : 3 * units, pl.ds(at, half)]
    rows, far = mine[...], other[...]
    gate = mm(rows, gate_s[:, pl.ds(at, half)], NT) + mm(far, gate_s[:, pl.ds(back, half)], NT)
    up = mm(rows, up_s[:, pl.ds(at, half)], NT) + mm(far, up_s[:, pl.ds(back, half)], NT)
    out[...] = mm(clamped_unit(gate, up).astype(bf16), down_s[...])


def join_kernel(dense, mine, other, out, wide_s):
    total = (mine[...].astype(f32) + other[...].astype(f32)).astype(bf16).astype(f32)
    spread(wide_s, total, 0)
    spread(wide_s, dense[...], CAP)
    out[...] = wide_s[...].astype(bf16)


def home_kernel(home_map, returned, kept, row_gate, out, wide_s, rows_s):
    seqs, half = kept.shape
    parts = half // LANES
    peers = rows_s.shape[0] // SLOTS
    wide_s[...] = returned[...].astype(f32)
    for r in range(SLOTS):
        for c in range(parts):
            rows_s[r * peers : (r + 1) * peers, c * LANES : (c + 1) * LANES] = gather(
                wide_s, r, c, parts, peers
            )
    sums = mm(home_map[...], rows_s[...])
    out[...] = (kept[...] + sums[:seqs] + row_gate[:, 0:1] * sums[seqs:]).astype(bf16)


def swap(array):
    return lax.ppermute(array, "tp", [(0, 1), (1, 0)])


def across(array, turn):
    pairs = []
    for a in range(4):
        for b in range(4):
            for t in range(2):
                flip = (t + turn) % 2
                to = 4 * (a ^ (1 - flip)) + (b ^ flip)
                pairs.append((2 * (4 * a + b) + t, 2 * to + t))
    return lax.ppermute(array, ("ep_0", "ep_1", "tp"), pairs)


def shards(
    tokens, attn_gain, w_query1, w_query2, w_key1, w_key2, w_value, query_gain, key_gain,
    head_lambda, sub_gain, w_output, cache_key, cache_value, lengths, mix_gain, expert_gate,
    expert_up, expert_down, routes, route_weight, dense_mix, dense_gate, dense_up, dense_down,
):
    peers = lax.axis_size(EP)
    seqs, width = tokens.shape
    half, slots, wide = width // 2, CAP * peers, SLOTS * peers
    hidden = expert_gate.shape[2]
    units = dense_down.shape[0]
    (pack,) = call(
        pack_kernel,
        (dense_gate.T, dense_up.T, dense_down),
        [((3 * units, width), bf16)],
        [],
        1 << 34,
        far=3,
        sems=3,
    )
    pack0 = across(pack, 0)
    part, send_map, home_map = attention(
        tokens, attn_gain, w_query1, w_query2, w_key1, w_key2, w_value, query_gain,
        key_gain, head_lambda, sub_gain, w_output, cache_key, cache_value, lengths,
        routes, route_weight, peers,
    )
    block = (wide * half // LANES, LANES)
    far = swap(part)
    pack1 = across(pack, 1)
    pack2 = across(pack0, 1)
    send, kept, row_gate = call(
        mix_kernel,
        (
            tokens, part, far, mix_gain.reshape(1, -1),
            dense_mix.reshape(-1, LANES), send_map,
        ),
        [(block, bf16), ((seqs, half), f32), ((seqs, LANES), f32)],
        [(block, f32)],
        2 * wide * seqs * half,
    )

    def exchange(blocks):
        blocks = blocks.reshape(peers, -1, LANES)
        return lax.all_to_all(blocks, EP, 0, 0, tiled=True).reshape(block)

    mine = exchange(send)
    other = swap(mine)
    rows_mine, gate_part, up_part = call(
        first_kernel,
        (mine, expert_gate, expert_up),
        [((DENSE_ROWS * peers, half), bf16)] + [((slots, hidden), f32)] * 2,
        [(block, f32), ((slots, half), bf16)],
        4 * slots * half * hidden,
    )
    rows_other, own, sent = call(
        second_kernel,
        (other, gate_part, up_part, expert_gate, expert_up, expert_down),
        [((DENSE_ROWS * peers, half), bf16)] + [((slots, half), bf16)] * 2,
        [(block, f32), ((slots, half), bf16), ((slots, width), f32)],
        8 * slots * half * hidden,
        slots * hidden,
    )
    came = swap(sent)
    packs = [pack, pack0, pack1, pack2]
    packs = packs + [swap(one) for one in packs]
    units = pack.shape[0] // 3 * len(packs)
    (dense,) = call(
        dense_kernel,
        (rows_mine, rows_other, *packs),
        [((DENSE_ROWS * peers, half), f32)],
        [((units, width), bf16), ((units, width), bf16), ((units, half), bf16)],
        10 * DENSE_ROWS * peers * half * units,
        DENSE_ROWS * peers * units,
    )
    (joined,) = call(join_kernel, (dense, own, came), [(block, bf16)], [(block, f32)], 0)
    returned = exchange(joined)
    (out,) = call(
        home_kernel,
        (home_map, returned, kept, row_gate),
        [((seqs, half), bf16)],
        [(block, f32), ((wide, half), bf16)],
        4 * seqs * wide * half,
    )
    return out


def solution(mesh):
    torus = Mesh(mesh.devices.reshape(4, 4, 4, mesh.shape["tp"]), EP_TP)
    in_specs = (
        P(EP, None), P(), P(None, "tp"), P(None, "tp"), P(None, "tp"), P(None, "tp"),
        P(None, "tp"), P(), P(), P("tp"), P(), P("tp", None), P(EP, "tp", None, None),
        P(EP, "tp", None, None), P(EP), P(), P(EP, None, "tp"), P(EP, None, "tp"),
        P(EP, "tp", None), P(EP, None), P(EP, None), P(), P(None, EP_TP), P(None, EP_TP),
        P(EP_TP, None),
    )
    return jax.shard_map(
        shards, mesh=torus, in_specs=in_specs, out_specs=P(EP, "tp"), check_vma=False
    )
```
